32 devices in a mesh: ep: 8 (over z, y), tp: 4 (over x, core).
Axes of the slice: x: 2, y: 2, z: 4, core: 2. Of those that a mesh axis runs over, the one named last changes fastest.
Arguments:
- mixer_input: bfloat16 [4096, 2048], P(('ep', 'tp')), may hold values from -6 to 6
- expert_input: bfloat16 [4096, 2048], P(('ep', 'tp')), may hold values from -6 to 6
- mixer_gain: float32 [2048], replicated, may hold values from 0.1 to 1.9
- expert_gain: float32 [2048], replicated, may hold values from 0.1 to 1.9
- query_weight: bfloat16 [2048, 1024], P(None, 'tp'), may hold values from -0.125 to 0.125
- key_weight: bfloat16 [2048, 1024], P(None, 'tp'), may hold values from -0.125 to 0.125
- value_weight: bfloat16 [2048, 1024], P(None, 'tp'), may hold values from -0.125 to 0.125
- out_weight: bfloat16 [1024, 2048], P('tp'), may hold values from -0.1875 to 0.1875
- decay_rate: float32 [8], P('tp'), may hold values from 0 to 0.12
- routing: int32 [4096, 4], P('ep'), may hold values from 0 to 7, all different within a row; in each aligned block of 128 rows (0 to 127, 128 to 255, ...) at most 96 rows name the same one
- route_weight: float32 [4096, 4], P('ep'), may hold values from 0.2 to 1
- gate_weight: bfloat16 [8, 2048, 1024], P('ep', None, 'tp'), may hold values from -0.125 to 0.125
- up_weight: bfloat16 [8, 2048, 1024], P('ep', None, 'tp'), may hold values from -0.125 to 0.125
- down_weight: bfloat16 [8, 1024, 2048], P('ep', None, 'tp'), may hold values from -0.1875 to 0.1875
- shared_gate: bfloat16 [2048, 512], P(None, 'tp'), may hold values from -0.125 to 0.125
- shared_up: bfloat16 [2048, 512], P(None, 'tp'), may hold values from -0.125 to 0.125
- shared_down: bfloat16 [512, 2048], P(None, 'tp'), may hold values from -0.25 to 0.25
Outputs:
- mixer_output: float32 [4096, 2048], P(('ep', 'tp'))
- expert_output: float32 [4096, 2048], P('ep', 'tp')
The draws below stay inside these ranges and needn't reach their ends.
Inputs may be any that keep to these rules, and one draw needn't show every extreme that they name: `routing`: each row names 4 different experts. In each aligned block of 128 rows, no expert is named by more than 96 rows, and in some blocks one expert is named by exactly 96 rows.
All inputs are finite; a program needn't handle non-finite values.
Results may differ from the reference program's by a relative error of at most 0.0095.
Values may be sent and summed in bfloat16 or wider, within the bound.
No kernel may reach another device: no remote copies, remote signals or barrier semaphores. Data moves between devices by JAX's collectives and lax.ppermute only.
A program may use at most 128 MiB of HBM per device.

```python
import math
import jax
import jax.numpy as jnp
import numpy as np
from jax import lax

D = 2048
HEADS = 8
HD = 128
F = 1024
FS = 512
K = 4
BLK = 64
R = 128
TOKENS = 4096
EXPERTS = 8
CAP = 96
N_EP = 8
N_TP = 4


def draw_decay_rate(key, part):
    order_key = jax.random.fold_in(key, 11)
    slow_key = jax.random.fold_in(key, 12)
    fast_key = jax.random.fold_in(key, 13)
    ranking = jax.random.permutation(order_key, HEADS)
    fast_count = HEADS // 2
    is_fast = ranking < fast_count
    slow_rate = jnp.exp(jax.random.uniform(slow_key, (HEADS,), jnp.float32, math.log(0.05), 0.0)) * (math.log(10.0) / TOKENS)
    quick_decay_rate = jax.random.uniform(fast_key, (HEADS,), jnp.float32, 0.05, 0.12)
    return jnp.where(is_fast, quick_decay_rate, slow_rate).astype(jnp.float32)


def block_levels(key, extent, split, low, top_value):
    gain, own = 1.0, jax.random.fold_in(key, 6)
    for position, shards_of in split:
        heights = jnp.exp(jax.random.uniform(jax.random.fold_in(own, position), (shards_of,), jnp.float32, low / len(split), top_value / len(split)))
        gain = gain * jnp.repeat(heights, extent[position] // shards_of).reshape([-1 if axis == position else 1 for axis in range(len(extent))])
    return gain


def assign_block(rng, own, number, rows, count, top, bound, skew):
    order = jax.random.permutation(rng, count)
    heavy_load, ordinary = shares(count, rows * top, bound, skew, True), shares(count, rows * top, bound, skew, False)
    places = jnp.arange(count)

    def named(tallies, rotation):
        used = int((tallies > 0).sum())
        fixed = max(1, used // 4)
        moved = fixed + (places - fixed + rotation * (used - fixed)) % max(1, count - fixed)
        return jnp.zeros((count,), jnp.int32).at[order[jnp.where(places < fixed, places, moved)]].set(jnp.asarray(tallies, jnp.int32))

    tallies = jnp.where(number % 4 == 0, named(heavy_load, number // 4), named(ordinary, number - number // 4 - 1))
    mixed = jax.random.permutation(jax.random.fold_in(own, 3), count)
    source_of, receiver = mixed[0:count // 2 * 2:2], mixed[1:count // 2 * 2:2]
    margin = jnp.minimum(tallies[source_of] - 1, bound - tallies[receiver]) // 2
    margin = jnp.where((source_of == order[0]) | (receiver == order[0]) | (tallies[receiver] == 0), 0, jnp.maximum(margin, 0))
    moved = jax.random.randint(jax.random.fold_in(own, 4), (count // 2,), 0, 1 << 20) % (margin + 1)
    tallies = tallies.at[source_of].add(-moved).at[receiver].add(moved)
    items = jnp.searchsorted(jnp.cumsum(tallies), jnp.arange(rows * top), side="right").astype(jnp.int32)
    grid = items.reshape(top, rows).T
    grid = grid[jax.random.permutation(jax.random.fold_in(own, 1), rows)]
    rotation = jax.random.randint(jax.random.fold_in(own, 2), (rows, 1), 0, top)
    return jnp.take_along_axis(grid, (jnp.arange(top)[None, :] + rotation) % top, axis=1)


def shares(number_of, total, bound, skew, full):
    portions = [(1 << 20) // math.isqrt(grade ** skew) + 1 for grade in range(1, number_of + 1)]
    largest = bound if full else min(bound, max(-(-total // number_of), total * portions[0] // sum(portions)))
    least = 1 if total - largest >= number_of - 1 else 0
    counts, rest = [largest] + [least] * (number_of - 1), total - largest - least * (number_of - 1)
    while rest > 0:
        movable = [i for i in range(1, number_of) if counts[i] < largest] or [i for i in range(1, number_of) if counts[i] < bound]
        mass, budget = sum([portions[i] for i in movable]), rest
        for i in movable:
            more = min(bound - counts[i], max(1, budget * portions[i] // mass), rest)
            counts[i] = counts[i] + more
            rest = rest - more
    return np.array(counts)


def gaussian(key, dims, spread, most, shards=(), kind=jnp.bfloat16):
    array = jax.random.normal(key, dims, jnp.float32) * spread
    if len(shards) > 0:
        array = block_levels(key, dims, shards, -0.22, 0.18) * array
    return jnp.clip(array, min=-most, max=most).astype(kind)


def setup_inputs(seed: int = 0) -> dict:
    key_list = jax.random.split(jax.random.key(seed), 18)
    mixer_input = gaussian(key_list[0], (TOKENS, D), 1.0, 6.0, ((0, 32),))
    expert_input = gaussian(key_list[1], (TOKENS, D), 1.0, 6.0, ((0, 32),))
    mixer_gain = jnp.clip(1.0 + 0.18 * jax.random.normal(key_list[2], (D,), jnp.float32), 0.1, 1.9)
    expert_gain = jnp.clip(1.0 + 0.18 * jax.random.normal(key_list[3], (D,), jnp.float32), 0.1, 1.9)
    query_weight = gaussian(key_list[4], (D, HEADS * HD), D ** -0.5, 0.125, ((1, 4),))
    key_weight = gaussian(key_list[5], (D, HEADS * HD), D ** -0.5, 0.125, ((1, 4),))
    value_weight = gaussian(key_list[6], (D, HEADS * HD), D ** -0.5, 0.125, ((1, 4),))
    out_weight = gaussian(key_list[7], (HEADS * HD, D), (HEADS * HD) ** -0.5, 0.1875, ((0, 4),))
    decay_rate = draw_decay_rate(jax.random.fold_in(key_list[17], 71), 0)
    routing_keys = jax.random.split(jax.random.fold_in(key_list[9], 1), TOKENS // R)
    routing_turns = jax.random.permutation(jax.random.fold_in(key_list[9], 3), TOKENS // R)
    routing = jax.vmap(lambda own, number: assign_block(jax.random.fold_in(key_list[9], 2), own, number, R, EXPERTS, K, CAP, 1))(routing_keys, routing_turns).reshape((TOKENS, K))
    route_weight = jnp.clip(0.2 + 0.8 * jax.random.uniform(key_list[10], (TOKENS, K), jnp.float32) ** block_levels(key_list[10], (TOKENS, K), ((0, 8),), -0.2, 0.2), 0.2, 1.0)
    gate_weight = gaussian(key_list[11], (EXPERTS, D, F), D ** -0.5, 0.125, ((0, 8), (2, 4)))
    up_weight = gaussian(key_list[12], (EXPERTS, D, F), D ** -0.5, 0.125, ((0, 8), (2, 4)))
    down_weight = gaussian(key_list[13], (EXPERTS, F, D), F ** -0.5, 0.1875, ((0, 8), (2, 4)))
    shared_gate = gaussian(key_list[14], (D, FS), D ** -0.5, 0.125, ((1, 4),))
    shared_up = gaussian(key_list[15], (D, FS), D ** -0.5, 0.125, ((1, 4),))
    shared_down = gaussian(key_list[16], (FS, D), FS ** -0.5, 0.25, ((1, 4),))
    return dict(mixer_input=mixer_input, expert_input=expert_input, mixer_gain=mixer_gain, expert_gain=expert_gain, query_weight=query_weight, key_weight=key_weight, value_weight=value_weight, out_weight=out_weight, decay_rate=decay_rate, routing=routing, route_weight=route_weight, gate_weight=gate_weight, up_weight=up_weight, down_weight=down_weight, shared_gate=shared_gate, shared_up=shared_up, shared_down=shared_down)


NORM_EPS = 1e-06
ROPE_BASE = 10000.0
EXACT_MATMUL = lax.Precision.HIGHEST

def norm_rows(inputs, gain_vector):
    values = inputs.astype(jnp.float32)
    scaled = values * lax.rsqrt(lax.optimization_barrier(jnp.mean(values * values, axis=-1, keepdims=True)) + NORM_EPS)
    return (scaled * gain_vector.astype(jnp.float32)).astype(jnp.bfloat16)

def rotate(head_rows, positions):
    head_size = head_rows.shape[-1]
    inverse = ROPE_BASE ** (-jnp.arange(0, head_size, 2, dtype=jnp.float32) / head_size)
    angles = positions[:, None] * inverse[None, :]
    cosine = jnp.cos(angles)[:, None, :]
    sine_part = jnp.sin(angles)[:, None, :]
    front_half = head_rows[..., :head_size // 2]
    behind = head_rows[..., head_size // 2:]
    return jnp.concatenate([front_half * cosine - behind * sine_part, front_half * sine_part + behind * cosine], axis=-1)

def project(inputs, weight):
    product = jnp.dot(inputs, weight, preferred_element_type=jnp.float32).astype(jnp.bfloat16)
    product = lax.optimization_barrier(product)
    return product.astype(jnp.float32).reshape(inputs.shape[0], HEADS, HD)

def retention_scan(query_heads, key_heads, value_heads, decay_rates):
    length = query_heads.shape[0]
    blocks = length // BLK
    log_gamma = -decay_rates.astype(jnp.float32)
    inner_pos = jnp.arange(BLK, dtype=jnp.float32)
    offsets = inner_pos[:, None] - inner_pos[None, :]
    inside_block_output = jnp.where(offsets >= 0, jnp.exp(log_gamma[:, None, None] * jnp.maximum(offsets, 0.0)), 0.0)
    key_scale = jnp.exp(log_gamma[None, :] * (BLK - 1.0 - inner_pos)[:, None])
    query_scale = jnp.exp(log_gamma[None, :] * (inner_pos + 1.0)[:, None])
    through = jnp.exp(log_gamma * BLK)

    def advance(carried, block_in):
        query_block_slice, key_block_slice, v_block = block_in
        attention_scores = jnp.einsum('ayr,iyr->yai', query_block_slice, key_block_slice, precision=EXACT_MATMUL) * inside_block_output
        nearby = jnp.einsum('hcm,mhe->che', attention_scores, v_block, precision=EXACT_MATMUL)
        distant = jnp.einsum('chd,hde->che', query_block_slice * query_scale[:, :, None], carried, precision=EXACT_MATMUL)
        update = jnp.einsum('chd,che->hde', key_block_slice * key_scale[:, :, None], v_block, precision=EXACT_MATMUL)
        return (through[:, None, None] * carried + update, nearby + distant)
    blocked = (blocks, BLK, HEADS, HD)
    _, outputs = lax.scan(advance, jnp.zeros((HEADS, HD, HD), jnp.float32), (query_heads.reshape(blocked), key_heads.reshape(blocked), value_heads.reshape(blocked)))
    return outputs.reshape(length, HEADS, HD)

def reference(mixer_input, expert_input, mixer_gain, expert_gain, query_weight, key_weight, value_weight, out_weight, decay_rate, routing, route_weight, gate_weight, up_weight, down_weight, shared_gate, shared_up, shared_down):
    mixer_rows = norm_rows(mixer_input, mixer_gain)
    positions = jnp.arange(TOKENS, dtype=jnp.float32)
    query_heads = rotate(project(mixer_rows, query_weight), positions) * HD ** (-0.5)
    key_heads = rotate(project(mixer_rows, key_weight), positions)
    value_heads = project(mixer_rows, value_weight)
    retained = retention_scan(query_heads, key_heads, value_heads, decay_rate)
    normed = retained * lax.rsqrt(lax.optimization_barrier(jnp.mean(retained * retained, axis=-1, keepdims=True)) + NORM_EPS)
    mixed_heads = normed.astype(jnp.bfloat16).reshape(TOKENS, HEADS * HD)
    group_width = HEADS * HD // N_TP
    summed_out = jnp.zeros((TOKENS, D), jnp.float32)
    for group_id in range(N_TP):
        partial_out = jnp.dot(mixed_heads[:, group_id * group_width:(group_id + 1) * group_width], out_weight[group_id * group_width:(group_id + 1) * group_width], preferred_element_type=jnp.float32).astype(jnp.bfloat16)
        summed_out = summed_out + lax.optimization_barrier(partial_out).astype(jnp.float32)
    mixer_output = summed_out
    expert_rows = norm_rows(expert_input, expert_gain)
    assigned = TOKENS * K
    chosen = routing.reshape(assigned).astype(jnp.int32)
    onehot = (chosen[:, None] == jnp.arange(EXPERTS, dtype=jnp.int32)[None, :]).astype(jnp.int32)
    ranks = lax.optimization_barrier(jnp.sum((jnp.cumsum(onehot, axis=0) - onehot) * onehot, axis=1)).astype(jnp.int32)
    owners = (jnp.arange(assigned, dtype=jnp.int32) // K + 1).astype(jnp.int32)
    room_size = N_EP * N_TP * CAP
    owner_table = jnp.zeros((EXPERTS, room_size), jnp.int32).at[chosen, ranks].set(owners)
    weight_table = jnp.zeros((EXPERTS, room_size), jnp.float32).at[chosen, ranks].set(route_weight.reshape(assigned).astype(jnp.float32))
    padded = jnp.concatenate([jnp.zeros((1, D), jnp.bfloat16), expert_rows], axis=0)

    def one_expert(summed, inputs):
        owner_ids, scales, gate_part, up_part, down_part = inputs
        picked = padded[owner_ids]
        hidden = (jax.nn.silu(jnp.dot(picked, gate_part, preferred_element_type=jnp.float32)) * jnp.dot(picked, up_part, preferred_element_type=jnp.float32)).astype(jnp.bfloat16)
        result = jnp.dot(hidden, down_part, preferred_element_type=jnp.float32).astype(jnp.bfloat16)
        result = lax.optimization_barrier(result).astype(jnp.float32)
        return (summed.at[owner_ids].add(result * scales[:, None]), None)
    summed, _ = lax.scan(one_expert, jnp.zeros((TOKENS + 1, D), jnp.float32), (owner_table, weight_table, gate_weight, up_weight, down_weight))
    shared_hidden = (jax.nn.silu(jnp.dot(expert_rows, shared_gate, preferred_element_type=jnp.float32)) * jnp.dot(expert_rows, shared_up, preferred_element_type=jnp.float32)).astype(jnp.bfloat16)
    shared_result = jnp.dot(shared_hidden, shared_down, preferred_element_type=jnp.float32)
    expert_output = summed[1:] + shared_result
    return (mixer_output, expert_output)
```

```python
import jax
import jax.numpy as jnp
from jax import lax
from jax.sharding import PartitionSpec as P

HD = 128
BLK = 64


NORM_EPS = 1e-06
ROPE_BASE = 10000.0
EXACT_MATMUL = lax.Precision.HIGHEST


def prefix(part, axis, combine, identity):
    place = lax.axis_index(axis)
    gathered = jax.tree.map(lambda a: lax.all_gather(a, axis), part)
    state = jax.tree.map(lambda a, e: jnp.zeros_like(a) + jnp.asarray(e, a.dtype), part, identity)

    def one(turn, state):
        return combine(
            state, jax.tree.map(lambda a: lax.dynamic_index_in_dim(a, turn, 0, False), gathered)
        )

    return lax.fori_loop(0, place, one, state)


def norm_rows(inputs, gain_vector):
    values = inputs.astype(jnp.float32)
    scaled = values * lax.rsqrt(jnp.mean(values * values, axis=-1, keepdims=True) + NORM_EPS)
    return (scaled * gain_vector).astype(jnp.bfloat16)


def rotate(head_rows, positions):
    head_size = head_rows.shape[-1]
    inverse = ROPE_BASE ** (-jnp.arange(0, head_size, 2, dtype=jnp.float32) / head_size)
    angles = positions[:, None] * inverse[None, :]
    cosine = jnp.cos(angles)[:, None, :]
    sine_part = jnp.sin(angles)[:, None, :]
    front_half = head_rows[..., : head_size // 2]
    behind = head_rows[..., head_size // 2 :]
    return jnp.concatenate(
        [front_half * cosine - behind * sine_part, front_half * sine_part + behind * cosine],
        axis=-1,
    )


def project(inputs, weight, head_total):
    product = jnp.dot(inputs, weight, preferred_element_type=jnp.float32).astype(jnp.bfloat16)
    product = lax.optimization_barrier(product)
    return product.astype(jnp.float32).reshape(inputs.shape[0], head_total, -1)


def chain_combine(earlier, latter):
    return (earlier[0] * latter[0], latter[0][:, None, None] * earlier[1] + latter[1])


def retain_local(query_heads, key_heads, value_heads, decay_rates):
    length, head_total, head_size = query_heads.shape
    blocks = length // BLK
    log_gamma = -decay_rates
    inner_pos = jnp.arange(BLK, dtype=jnp.float32)
    offsets = inner_pos[:, None] - inner_pos[None, :]
    inside_block_output = jnp.where(
        offsets >= 0, jnp.exp(log_gamma[:, None, None] * jnp.maximum(offsets, 0.0)), 0.0
    )
    key_scale = jnp.exp(log_gamma[None, :] * (BLK - 1.0 - inner_pos)[:, None])
    query_scale = jnp.exp(log_gamma[None, :] * (inner_pos + 1.0)[:, None])
    blocked = (blocks, BLK, head_total, head_size)
    q_blocks = query_heads.reshape(blocked)
    k_blocks = key_heads.reshape(blocked)
    v_blocks = value_heads.reshape(blocked)
    attention_scores = (
        jnp.einsum("nchd,nmhd->nhcm", q_blocks, k_blocks, precision=EXACT_MATMUL)
        * inside_block_output[None]
    )
    nearby = jnp.einsum("nhcm,nmhe->nche", attention_scores, v_blocks, precision=EXACT_MATMUL)
    block_states = jnp.einsum(
        "nchd,nche->nhde", k_blocks * key_scale[None, :, :, None], v_blocks, precision=EXACT_MATMUL
    )
    block_offset_rows = jnp.arange(blocks, dtype=jnp.float32)
    to_end = jnp.exp(log_gamma[None, :] * BLK * (blocks - 1.0 - block_offset_rows)[:, None])
    summary = jnp.einsum("nh,nhde->hde", to_end, block_states, precision=EXACT_MATMUL)
    through = jnp.exp(log_gamma * (BLK * blocks))
    incoming = prefix(
        (through, summary), "ep", chain_combine, (jnp.ones_like(through), jnp.zeros_like(summary))
    )[1]
    block_gaps = block_offset_rows[:, None] - 1.0 - block_offset_rows[None, :]
    carry_mix = jnp.where(
        block_gaps >= 0, jnp.exp(log_gamma[:, None, None] * BLK * jnp.maximum(block_gaps, 0.0)), 0.0
    )
    entering = jnp.einsum("hbj,jhde->bhde", carry_mix, block_states, precision=EXACT_MATMUL)
    entering = (
        entering
        + jnp.exp(log_gamma[None, :] * BLK * block_offset_rows[:, None])[:, :, None, None]
        * incoming[None]
    )
    distant = jnp.einsum(
        "bchd,bhde->bche",
        q_blocks * query_scale[None, :, :, None],
        entering,
        precision=EXACT_MATMUL,
    )
    retained = (nearby + distant).reshape(length, head_total, head_size)
    normed = retained * lax.rsqrt(jnp.mean(retained * retained, axis=-1, keepdims=True) + NORM_EPS)
    return normed.astype(jnp.bfloat16).reshape(length, head_total * head_size)


def assign_slots(routes, source_rows, capacity, expert_count):
    token_count, pick_count = routes.shape
    chosen = routes.reshape(token_count * pick_count)
    onehot = (chosen[:, None] == jnp.arange(expert_count, dtype=jnp.int32)[None, :]).astype(
        jnp.int32
    )
    per_source = onehot.reshape(token_count // source_rows, source_rows * pick_count, expert_count)
    earlier_hits = jnp.cumsum(per_source, axis=1) - per_source
    ranks = jnp.sum(earlier_hits * per_source, axis=2).reshape(token_count * pick_count)
    sources = jnp.arange(token_count * pick_count, dtype=jnp.int32) // (source_rows * pick_count)
    return (chosen, sources * capacity + ranks)


def gather_slots(token_rows, chosen, slot_ids, slot_count, expert_count, pick_count):
    owners = jnp.arange(chosen.shape[0], dtype=jnp.int32) // pick_count + 1
    owner_table = jnp.zeros((slot_count, expert_count), jnp.int32).at[slot_ids, chosen].set(owners)
    padded = jnp.concatenate(
        [jnp.zeros((1, token_rows.shape[1]), token_rows.dtype), token_rows], axis=0
    )
    return padded[owner_table]


def expert_hidden(routed_rows, gate_weight, up_weight):
    per_device = gate_weight.shape[0]
    grouped = routed_rows.reshape(
        routed_rows.shape[0], routed_rows.shape[1] // per_device, per_device, routed_rows.shape[2]
    )
    gate_part = jnp.einsum(
        "snxd,xdf->snxf", grouped, gate_weight, preferred_element_type=jnp.float32
    )
    up_part = jnp.einsum("snxd,xdf->snxf", grouped, up_weight, preferred_element_type=jnp.float32)
    return (jax.nn.silu(gate_part) * up_part).astype(jnp.bfloat16)


def routed_shards(
    mixer_input,
    expert_input,
    mixer_gain,
    expert_gain,
    query_weight,
    key_weight,
    value_weight,
    out_weight,
    decay_rate,
    routing,
    route_weight,
    gate_weight,
    up_weight,
    down_weight,
    shared_gate,
    shared_up,
    shared_down,
):
    own_count = mixer_input.shape[0]
    tp_index = lax.axis_index("tp")
    own_expert_rows = norm_rows(expert_input, expert_gain)
    mixer_rows, expert_rows = (
        lax.all_gather(norm_rows(mixer_input, mixer_gain), "tp", axis=0, tiled=True),
        lax.all_gather(own_expert_rows, "tp", axis=0, tiled=True),
    )
    group_count = mixer_rows.shape[0]
    head_total = decay_rate.shape[0]
    positions = (
        lax.axis_index("ep") * group_count + jnp.arange(group_count, dtype=jnp.int32)
    ).astype(jnp.float32)
    query_heads = rotate(project(mixer_rows, query_weight, head_total), positions) * HD ** (-0.5)
    key_heads = rotate(project(mixer_rows, key_weight, head_total), positions)
    value_heads = project(mixer_rows, value_weight, head_total)
    mixed_heads = retain_local(query_heads, key_heads, value_heads, decay_rate)
    mixer_output = lax.psum_scatter(
        jnp.dot(mixed_heads, out_weight, preferred_element_type=jnp.float32).astype(jnp.bfloat16),
        "tp",
        scatter_dimension=0,
        tiled=True,
    ).astype(jnp.float32)
    expert_count = lax.axis_size("ep") * gate_weight.shape[0]
    pick_count = routing.shape[1]
    capacity = (3 * own_count * pick_count + 2 * expert_count - 1) // (2 * expert_count)
    chosen, slot_ids = assign_slots(routing, own_count, capacity, expert_count)
    own_span = own_count * pick_count
    own_chosen = lax.dynamic_slice_in_dim(chosen, tp_index * own_span, own_span, 0)
    own_slots = (
        lax.dynamic_slice_in_dim(slot_ids, tp_index * own_span, own_span, 0) - tp_index * capacity
    )
    outgoing = gather_slots(
        own_expert_rows, own_chosen, own_slots, capacity, expert_count, pick_count
    )
    arrived = lax.all_to_all(outgoing, "ep", split_axis=1, concat_axis=1, tiled=True)
    hidden = expert_hidden(
        lax.all_gather(arrived, "tp", axis=0, tiled=True), gate_weight, up_weight
    )
    shared_hidden = (
        jax.nn.silu(jnp.dot(expert_rows, shared_gate, preferred_element_type=jnp.float32))
        * jnp.dot(expert_rows, shared_up, preferred_element_type=jnp.float32)
    ).astype(jnp.bfloat16)
    full_hidden, full_shared = (
        lax.all_gather(hidden, "tp", axis=3, tiled=True),
        lax.all_gather(shared_hidden, "tp", axis=1, tiled=True),
    )
    results = jnp.einsum(
        "snxf,xfe->snxe", full_hidden, down_weight, preferred_element_type=jnp.float32
    ).astype(jnp.bfloat16)
    results = results.reshape(results.shape[0], expert_count, results.shape[3])
    returned = lax.all_to_all(results, "ep", split_axis=1, concat_axis=1, tiled=True)
    flat_results = returned.reshape(returned.shape[0] * expert_count, returned.shape[2])
    picked = flat_results[slot_ids * expert_count + chosen].astype(jnp.float32)
    weighted = jnp.sum(
        picked.reshape(group_count, pick_count, -1) * route_weight[:, :, None], axis=1
    )
    shared_result = jnp.dot(full_shared, shared_down, preferred_element_type=jnp.float32)
    expert_output = weighted + shared_result
    return (mixer_output, expert_output)


def exchange(value, step):
    size = lax.axis_size("tp")
    return lax.ppermute(value, "tp", [(i, i ^ step) for i in range(size)])


def tp_blocks(value):
    blocks = [value]
    step = lax.axis_size("tp") // 2
    if step == 0:
        return blocks
    held = {0: value}
    while step >= 1:
        held.update({k | step: exchange(v, step) for k, v in list(held.items())})
        step //= 2
    return [held[k] for k in range(lax.axis_size("tp"))]


def ring_order(size):
    return [i for i in range(0, size, 2)] + [i for i in range(size - 1, 0, -2)]


def ring_shift(value, step):
    size = lax.axis_size("ep")
    order = ring_order(size)
    return lax.ppermute(
        value, "ep", [(order[i], order[(i + step) % size]) for i in range(size)]
    )


def ring_gather(value):
    size = lax.axis_size("ep")
    half, rows = size // 2, value.shape[0] // 2
    held = {0: value}
    ahead = behind = value
    for d in range(1, half):
        behind = ring_shift(behind, 1)
        ahead = ring_shift(ahead, -1)
        held[size - d] = behind
        held[d] = ahead
    held[half] = jnp.concatenate(
        [ring_shift(behind[:rows], 1), ring_shift(ahead[rows:], -1)], axis=0
    )
    return [held[d] for d in range(size)]


def ring_scatter(parts):
    size = lax.axis_size("ep")
    half, rows = size // 2, parts[0].shape[0] // 2
    f32 = jnp.float32
    right = ring_shift(parts[half][:rows], 1)
    left = ring_shift(parts[half][rows:], -1)
    right = parts[half - 1].astype(f32).at[:rows].add(right.astype(f32)).astype(jnp.bfloat16)
    left = parts[half + 1].astype(f32).at[rows:].add(left.astype(f32)).astype(jnp.bfloat16)
    for d in range(half - 1, 0, -1):
        right, left = ring_shift(right, 1), ring_shift(left, -1)
        if d > 1:
            right = (right.astype(f32) + parts[d - 1].astype(f32)).astype(jnp.bfloat16)
            left = (left.astype(f32) + parts[size - d + 1].astype(f32)).astype(jnp.bfloat16)
    return parts[0].astype(f32) + right.astype(f32) + left.astype(f32)


def state_before(summary, through):
    size = lax.axis_size("ep")

    def from_earlier(value, step):
        return lax.ppermute(value, "ep", [(i, i + step) for i in range(size - step)])

    state = from_earlier(summary, 1)
    step, decay = 1, through[:, None, None]
    while step < size - 1:
        state = state + decay * from_earlier(state, step)
        step, decay = step * 2, decay * decay
    return state


def natural_rows(blocks, tp_index):
    rows = blocks[0].shape[0]
    total = jnp.zeros((rows * len(blocks),) + blocks[0].shape[1:], blocks[0].dtype)
    for k, block in enumerate(blocks):
        total = lax.dynamic_update_slice_in_dim(total, block, (tp_index ^ k) * rows, 0)
    return total


def natural_columns(blocks, tp_index):
    width = blocks[0].shape[1]
    total = jnp.zeros((blocks[0].shape[0], width * len(blocks)), blocks[0].dtype)
    for k, block in enumerate(blocks):
        total = lax.dynamic_update_slice_in_dim(total, block, (tp_index ^ k) * width, 1)
    return total


def gated(rows, gate, up):
    gate_part = jnp.dot(rows, gate, preferred_element_type=jnp.float32)
    up_part = jnp.dot(rows, up, preferred_element_type=jnp.float32)
    return (jax.nn.silu(gate_part) * up_part).astype(jnp.bfloat16)


def mixer(mixer_blocks, query_weight, key_weight, value_weight, out_weight, decay_rate):
    own_count = mixer_blocks[0].shape[0]
    block_count = len(mixer_blocks)
    group_count = own_count * block_count
    tp_index = lax.axis_index("tp")
    head_total = decay_rate.shape[0]
    rows = jnp.concatenate(mixer_blocks, axis=0)
    inner = jnp.concatenate(
        [(tp_index ^ k) * own_count + jnp.arange(own_count, dtype=jnp.int32) for k in range(block_count)]
    )
    positions = (lax.axis_index("ep") * group_count + inner).astype(jnp.float32)
    inner = inner.astype(jnp.float32)
    query_heads = rotate(project(rows, query_weight, head_total), positions) * HD ** (-0.5)
    key_heads = rotate(project(rows, key_weight, head_total), positions)
    value_heads = project(rows, value_weight, head_total)
    rate = decay_rate[:, None]
    key_scale = jnp.exp(-rate * (group_count - 1.0 - inner)[None, :])
    summary = jnp.einsum(
        "shd,she->hde", key_heads * key_scale.T[:, :, None], value_heads, precision=EXACT_MATMUL
    )
    incoming = state_before(summary, jnp.exp(-decay_rate * group_count))
    offsets = inner[:, None] - inner[None, :]
    decay = jnp.where(
        offsets >= 0, jnp.exp(-decay_rate[:, None, None] * jnp.maximum(offsets, 0.0)), 0.0
    )
    scores = jnp.einsum("phd,shd->hps", query_heads, key_heads, precision=EXACT_MATMUL) * decay
    nearby = jnp.einsum("hps,she->phe", scores, value_heads, precision=EXACT_MATMUL)
    query_scale = jnp.exp(-rate * (inner + 1.0)[None, :])
    distant = jnp.einsum(
        "phd,hde->phe", query_heads * query_scale.T[:, :, None], incoming, precision=EXACT_MATMUL
    )
    retained = nearby + distant
    normed = retained * lax.rsqrt(jnp.mean(retained * retained, axis=-1, keepdims=True) + NORM_EPS)
    mixed = normed.astype(jnp.bfloat16).reshape(group_count, head_total * retained.shape[2])
    product = jnp.dot(mixed, out_weight, preferred_element_type=jnp.float32).astype(jnp.bfloat16)
    parts = {k: product[k * own_count : (k + 1) * own_count] for k in range(block_count)}
    step = 1
    while step < block_count:
        kept = {}
        for k in parts:
            if not k & step:
                arrived = exchange(parts[k | step], step)
                total = parts[k].astype(jnp.float32) + arrived.astype(jnp.float32)
                kept[k] = total.astype(jnp.bfloat16) if 2 * step < block_count else total
        parts, step = kept, step * 2
    return parts[0].astype(jnp.float32)


def dense_shards(
    mixer_input,
    expert_input,
    mixer_gain,
    expert_gain,
    query_weight,
    key_weight,
    value_weight,
    out_weight,
    decay_rate,
    routing,
    route_weight,
    gate_weight,
    up_weight,
    down_weight,
    shared_gate,
    shared_up,
    shared_down,
):
    own_count = mixer_input.shape[0]
    tp_index = lax.axis_index("tp")
    ep_size, tp_size = lax.axis_size("ep"), lax.axis_size("tp")
    mixer_blocks = tp_blocks(norm_rows(mixer_input, mixer_gain))
    own_rows = norm_rows(expert_input, expert_gain)
    arrived = ring_gather(own_rows)
    gates, ups = tp_blocks(gate_weight[0]), tp_blocks(up_weight[0])
    downs = tp_blocks(down_weight[0])
    shared_rows = tp_blocks(own_rows)

    own_routes = lax.dynamic_slice_in_dim(routing, tp_index * own_count, own_count, 0)
    own_weights = lax.dynamic_slice_in_dim(route_weight, tp_index * own_count, own_count, 0)
    named = own_routes[None] == jnp.arange(ep_size, dtype=jnp.int32)[:, None, None]
    by_expert = jnp.sum(jnp.where(named, own_weights[None], 0.0), axis=2)
    by_source = lax.all_to_all(by_expert, "ep", split_axis=0, concat_axis=0, tiled=True)
    order = jnp.array(ring_order(ep_size), jnp.int32)
    ep_index = lax.axis_index("ep")
    place = jnp.where(ep_index % 2 == 0, ep_index // 2, ep_size - 1 - ep_index // 2)
    scales = by_source[order[(place + jnp.arange(ep_size)) % ep_size]].reshape(-1)

    mixer_output = mixer(
        mixer_blocks, query_weight, key_weight, value_weight, out_weight, decay_rate
    )

    tokens = jnp.concatenate(arrived, axis=0)
    hidden = natural_columns([gated(tokens, g, u) for g, u in zip(gates, ups)], tp_index)
    finals = []
    for k in range(tp_size):
        result = jnp.dot(hidden, downs[k], preferred_element_type=jnp.float32)
        result = (result * scales[:, None]).astype(jnp.bfloat16)
        total = ring_scatter(
            [result[d * own_count : (d + 1) * own_count] for d in range(ep_size)]
        ).astype(jnp.bfloat16)
        finals.append(total if k == 0 else exchange(total, k))

    shared_hidden = gated(jnp.concatenate(shared_rows, axis=0), shared_gate, shared_up)
    columns = []
    for m in range(tp_size):
        piece = shared_hidden if m == 0 else exchange(shared_hidden, m)
        columns.append(
            jnp.concatenate(
                [piece[(k ^ m) * own_count : ((k ^ m) + 1) * own_count] for k in range(tp_size)]
            )
        )
    shared_result = jnp.dot(
        natural_columns(columns, tp_index), shared_down, preferred_element_type=jnp.float32
    )
    outputs = [
        finals[k].astype(jnp.float32) + shared_result[k * own_count : (k + 1) * own_count]
        for k in range(tp_size)
    ]
    return (mixer_output, natural_rows(outputs, tp_index))


def shards(*arrays):
    own_count, pick_count = arrays[0].shape[0], arrays[9].shape[1]
    per_device = arrays[11].shape[0]
    ep_size, tp_size = lax.axis_size("ep"), lax.axis_size("tp")
    capacity = (3 * own_count * pick_count + 2 * ep_size - 1) // (2 * ep_size)
    dense = per_device == 1 and 2 * capacity >= own_count and ep_size % 2 == 0 and ep_size > 2
    if dense and tp_size & (tp_size - 1) == 0:
        return dense_shards(*arrays)
    return routed_shards(*arrays)


def solution(mesh):
    return jax.shard_map(
        shards,
        mesh=mesh,
        in_specs=(
            P(("ep", "tp"), None),
            P(("ep", "tp"), None),
            P(),
            P(),
            P(None, "tp"),
            P(None, "tp"),
            P(None, "tp"),
            P("tp", None),
            P("tp"),
            P("ep", None),
            P("ep", None),
            P("ep", None, "tp"),
            P("ep", None, "tp"),
            P("ep", None, "tp"),
            P(None, "tp"),
            P(None, "tp"),
            P(None, "tp"),
        ),
        out_specs=(P(("ep", "tp"), None), P("ep", "tp")),
        check_vma=False,
    )
```

```python
import functools

import jax
import jax.numpy as jnp
from jax import lax
from jax.experimental import pallas as pl
from jax.experimental.pallas import tpu as pltpu
from jax.sharding import PartitionSpec as P


HD = 128
BLK = 64


NORM_EPS = 1e-06
ROPE_BASE = 10000.0
EXACT_MATMUL = lax.Precision.HIGHEST


def prefix(part, axis, combine, identity):
    place = lax.axis_index(axis)
    gathered = jax.tree.map(lambda a: lax.all_gather(a, axis), part)
    state = jax.tree.map(lambda a, e: jnp.zeros_like(a) + jnp.asarray(e, a.dtype), part, identity)

    def one(turn, state):
        return combine(
            state, jax.tree.map(lambda a: lax.dynamic_index_in_dim(a, turn, 0, False), gathered)
        )

    return lax.fori_loop(0, place, one, state)


def norm_rows(inputs, gain_vector):
    values = inputs.astype(jnp.float32)
    scaled = values * lax.rsqrt(jnp.mean(values * values, axis=-1, keepdims=True) + NORM_EPS)
    return (scaled * gain_vector).astype(jnp.bfloat16)


def rotate(head_rows, positions):
    head_size = head_rows.shape[-1]
    inverse = ROPE_BASE ** (-jnp.arange(0, head_size, 2, dtype=jnp.float32) / head_size)
    angles = positions[:, None] * inverse[None, :]
    cosine = jnp.cos(angles)[:, None, :]
    sine_part = jnp.sin(angles)[:, None, :]
    front_half = head_rows[..., : head_size // 2]
    behind = head_rows[..., head_size // 2 :]
    return jnp.concatenate(
        [front_half * cosine - behind * sine_part, front_half * sine_part + behind * cosine],
        axis=-1,
    )


def project(inputs, weight, head_total):
    product = jnp.dot(inputs, weight, preferred_element_type=jnp.float32).astype(jnp.bfloat16)
    product = lax.optimization_barrier(product)
    return product.astype(jnp.float32).reshape(inputs.shape[0], head_total, -1)


def chain_combine(earlier, latter):
    return (earlier[0] * latter[0], latter[0][:, None, None] * earlier[1] + latter[1])


def retain_local(query_heads, key_heads, value_heads, decay_rates):
    length, head_total, head_size = query_heads.shape
    blocks = length // BLK
    log_gamma = -decay_rates
    inner_pos = jnp.arange(BLK, dtype=jnp.float32)
    offsets = inner_pos[:, None] - inner_pos[None, :]
    inside_block_output = jnp.where(
        offsets >= 0, jnp.exp(log_gamma[:, None, None] * jnp.maximum(offsets, 0.0)), 0.0
    )
    key_scale = jnp.exp(log_gamma[None, :] * (BLK - 1.0 - inner_pos)[:, None])
    query_scale = jnp.exp(log_gamma[None, :] * (inner_pos + 1.0)[:, None])
    blocked = (blocks, BLK, head_total, head_size)
    q_blocks = query_heads.reshape(blocked)
    k_blocks = key_heads.reshape(blocked)
    v_blocks = value_heads.reshape(blocked)
    attention_scores = (
        jnp.einsum("nchd,nmhd->nhcm", q_blocks, k_blocks, precision=EXACT_MATMUL)
        * inside_block_output[None]
    )
    nearby = jnp.einsum("nhcm,nmhe->nche", attention_scores, v_blocks, precision=EXACT_MATMUL)
    block_states = jnp.einsum(
        "nchd,nche->nhde", k_blocks * key_scale[None, :, :, None], v_blocks, precision=EXACT_MATMUL
    )
    block_offset_rows = jnp.arange(blocks, dtype=jnp.float32)
    to_end = jnp.exp(log_gamma[None, :] * BLK * (blocks - 1.0 - block_offset_rows)[:, None])
    summary = jnp.einsum("nh,nhde->hde", to_end, block_states, precision=EXACT_MATMUL)
    through = jnp.exp(log_gamma * (BLK * blocks))
    incoming = prefix(
        (through, summary), "ep", chain_combine, (jnp.ones_like(through), jnp.zeros_like(summary))
    )[1]
    block_gaps = block_offset_rows[:, None] - 1.0 - block_offset_rows[None, :]
    carry_mix = jnp.where(
        block_gaps >= 0, jnp.exp(log_gamma[:, None, None] * BLK * jnp.maximum(block_gaps, 0.0)), 0.0
    )
    entering = jnp.einsum("hbj,jhde->bhde", carry_mix, block_states, precision=EXACT_MATMUL)
    entering = (
        entering
        + jnp.exp(log_gamma[None, :] * BLK * block_offset_rows[:, None])[:, :, None, None]
        * incoming[None]
    )
    distant = jnp.einsum(
        "bchd,bhde->bche",
        q_blocks * query_scale[None, :, :, None],
        entering,
        precision=EXACT_MATMUL,
    )
    retained = (nearby + distant).reshape(length, head_total, head_size)
    normed = retained * lax.rsqrt(jnp.mean(retained * retained, axis=-1, keepdims=True) + NORM_EPS)
    return normed.astype(jnp.bfloat16).reshape(length, head_total * head_size)


def assign_slots(routes, source_rows, capacity, expert_count):
    token_count, pick_count = routes.shape
    chosen = routes.reshape(token_count * pick_count)
    onehot = (chosen[:, None] == jnp.arange(expert_count, dtype=jnp.int32)[None, :]).astype(
        jnp.int32
    )
    per_source = onehot.reshape(token_count // source_rows, source_rows * pick_count, expert_count)
    earlier_hits = jnp.cumsum(per_source, axis=1) - per_source
    ranks = jnp.sum(earlier_hits * per_source, axis=2).reshape(token_count * pick_count)
    sources = jnp.arange(token_count * pick_count, dtype=jnp.int32) // (source_rows * pick_count)
    return (chosen, sources * capacity + ranks)


def gather_slots(token_rows, chosen, slot_ids, slot_count, expert_count, pick_count):
    owners = jnp.arange(chosen.shape[0], dtype=jnp.int32) // pick_count + 1
    owner_table = jnp.zeros((slot_count, expert_count), jnp.int32).at[slot_ids, chosen].set(owners)
    padded = jnp.concatenate(
        [jnp.zeros((1, token_rows.shape[1]), token_rows.dtype), token_rows], axis=0
    )
    return padded[owner_table]


def expert_hidden(routed_rows, gate_weight, up_weight):
    per_device = gate_weight.shape[0]
    grouped = routed_rows.reshape(
        routed_rows.shape[0], routed_rows.shape[1] // per_device, per_device, routed_rows.shape[2]
    )
    gate_part = jnp.einsum(
        "snxd,xdf->snxf", grouped, gate_weight, preferred_element_type=jnp.float32
    )
    up_part = jnp.einsum("snxd,xdf->snxf", grouped, up_weight, preferred_element_type=jnp.float32)
    return (jax.nn.silu(gate_part) * up_part).astype(jnp.bfloat16)


def routed_shards(
    mixer_input,
    expert_input,
    mixer_gain,
    expert_gain,
    query_weight,
    key_weight,
    value_weight,
    out_weight,
    decay_rate,
    routing,
    route_weight,
    gate_weight,
    up_weight,
    down_weight,
    shared_gate,
    shared_up,
    shared_down,
):
    own_count = mixer_input.shape[0]
    tp_index = lax.axis_index("tp")
    own_expert_rows = norm_rows(expert_input, expert_gain)
    mixer_rows, expert_rows = (
        lax.all_gather(norm_rows(mixer_input, mixer_gain), "tp", axis=0, tiled=True),
        lax.all_gather(own_expert_rows, "tp", axis=0, tiled=True),
    )
    group_count = mixer_rows.shape[0]
    head_total = decay_rate.shape[0]
    positions = (
        lax.axis_index("ep") * group_count + jnp.arange(group_count, dtype=jnp.int32)
    ).astype(jnp.float32)
    query_heads = rotate(project(mixer_rows, query_weight, head_total), positions) * HD ** (-0.5)
    key_heads = rotate(project(mixer_rows, key_weight, head_total), positions)
    value_heads = project(mixer_rows, value_weight, head_total)
    mixed_heads = retain_local(query_heads, key_heads, value_heads, decay_rate)
    mixer_output = lax.psum_scatter(
        jnp.dot(mixed_heads, out_weight, preferred_element_type=jnp.float32).astype(jnp.bfloat16),
        "tp",
        scatter_dimension=0,
        tiled=True,
    ).astype(jnp.float32)
    expert_count = lax.axis_size("ep") * gate_weight.shape[0]
    pick_count = routing.shape[1]
    capacity = (3 * own_count * pick_count + 2 * expert_count - 1) // (2 * expert_count)
    chosen, slot_ids = assign_slots(routing, own_count, capacity, expert_count)
    own_span = own_count * pick_count
    own_chosen = lax.dynamic_slice_in_dim(chosen, tp_index * own_span, own_span, 0)
    own_slots = (
        lax.dynamic_slice_in_dim(slot_ids, tp_index * own_span, own_span, 0) - tp_index * capacity
    )
    outgoing = gather_slots(
        own_expert_rows, own_chosen, own_slots, capacity, expert_count, pick_count
    )
    arrived = lax.all_to_all(outgoing, "ep", split_axis=1, concat_axis=1, tiled=True)
    hidden = expert_hidden(
        lax.all_gather(arrived, "tp", axis=0, tiled=True), gate_weight, up_weight
    )
    shared_hidden = (
        jax.nn.silu(jnp.dot(expert_rows, shared_gate, preferred_element_type=jnp.float32))
        * jnp.dot(expert_rows, shared_up, preferred_element_type=jnp.float32)
    ).astype(jnp.bfloat16)
    full_hidden, full_shared = (
        lax.all_gather(hidden, "tp", axis=3, tiled=True),
        lax.all_gather(shared_hidden, "tp", axis=1, tiled=True),
    )
    results = jnp.einsum(
        "snxf,xfe->snxe", full_hidden, down_weight, preferred_element_type=jnp.float32
    ).astype(jnp.bfloat16)
    results = results.reshape(results.shape[0], expert_count, results.shape[3])
    returned = lax.all_to_all(results, "ep", split_axis=1, concat_axis=1, tiled=True)
    flat_results = returned.reshape(returned.shape[0] * expert_count, returned.shape[2])
    picked = flat_results[slot_ids * expert_count + chosen].astype(jnp.float32)
    weighted = jnp.sum(
        picked.reshape(group_count, pick_count, -1) * route_weight[:, :, None], axis=1
    )
    shared_result = jnp.dot(full_shared, shared_down, preferred_element_type=jnp.float32)
    expert_output = weighted + shared_result
    return (mixer_output, expert_output)


BF16, F32 = jnp.bfloat16, jnp.float32
LANES = 128
WHOLE = pltpu.CompilerParams(vmem_limit_bytes=60 << 20)


def exchange(value, step):
    size = lax.axis_size("tp")
    return lax.ppermute(value, "tp", [(i, i ^ step) for i in range(size)])


def ring_order(size):
    return [i for i in range(0, size, 2)] + [i for i in range(size - 1, 0, -2)]


def ring_shift(value, step):
    size = lax.axis_size("ep")
    order = ring_order(size)
    return lax.ppermute(value, "ep", [(order[i], order[(i + step) % size]) for i in range(size)])


def tp_blocks(value):
    held = {0: value}
    step = lax.axis_size("tp") // 2
    while step >= 1:
        for k in list(held):
            held[k | step] = exchange(held[k], step)
        step //= 2
    return [held[k] for k in range(lax.axis_size("tp"))]


def ring_gather(value):
    size = lax.axis_size("ep")
    half, rows = size // 2, value.shape[0] // 2
    offsets, blocks = [0], [value]
    ahead = behind = value
    for d in range(1, half):
        behind = ring_shift(behind, 1)
        ahead = ring_shift(ahead, -1)
        offsets += [size - d, d]
        blocks += [behind, ahead]
    offsets.append(half)
    blocks.append(ring_shift(behind[:rows], 1))
    blocks.append(ring_shift(ahead[rows:], -1))
    return offsets, blocks


def ring_scatter(parts, way):
    size = lax.axis_size("ep")
    half = size // 2
    long, short = parts[half], parts[(-way * (half - 1)) % size]

    def added(first, second):
        return (first.astype(F32) + second.astype(F32)).astype(BF16)

    for d in range(half, 0, -1):
        long = ring_shift(long, way)
        if d > 1:
            short = ring_shift(short, -way)
        if d > 1:
            long = added(long, parts[(way * (d - 1)) % size])
        if d > 2:
            short = added(short, parts[(-way * (d - 2)) % size])
    return (parts[0].astype(F32) + long.astype(F32) + short.astype(F32)).astype(BF16)


def state_before(summary, decay_rate, group_count):
    size, place = lax.axis_size("ep"), lax.axis_index("ep")
    rate = decay_rate[:, None, None] * group_count
    state, total = jnp.zeros_like(summary), summary
    step = 1
    while step < size:
        other = lax.ppermute(total, "ep", [(i, i ^ step) for i in range(size)])
        later = (place & step) != 0
        inside = (place & (step - 1)).astype(F32)
        state = state + jnp.where(later, jnp.exp(-rate * inside) * other, 0.0)
        passed = jnp.exp(-rate * step)
        total = jnp.where(later, passed * other + total, passed * total + other)
        step *= 2
    return state


def natural(blocks, tp_index, axis):
    extent = blocks[0].shape[axis]
    shape = list(blocks[0].shape)
    shape[axis] = extent * len(blocks)
    total = jnp.zeros(shape, blocks[0].dtype)
    for k, block in enumerate(blocks):
        total = lax.dynamic_update_slice_in_dim(total, block, (tp_index ^ k) * extent, axis)
    return total


def gated(rows, gate, up):
    gate_part = jnp.dot(rows, gate, preferred_element_type=F32)
    up_part = jnp.dot(rows, up, preferred_element_type=F32)
    return (jax.nn.silu(gate_part) * up_part).astype(BF16)


def fetch(sources, targets, semaphores, first=0):
    copies = [
        pltpu.make_async_copy(source, target, semaphores.at[first + i])
        for i, (source, target) in enumerate(zip(sources, targets))
    ]
    for copy in copies:
        copy.start()
    return copies


def row_views(ref, blocks, start=0):
    views = []
    for block in blocks:
        views.append(ref.at[pl.ds(start, block.shape[0])])
        start += block.shape[0]
    return views


def tiles_of(blocks):
    runs, start, low, members = [], 0, 0, []
    for number, block in enumerate(blocks):
        members.append(number)
        start += block.shape[0]
        left = sum(b.shape[0] for b in blocks[number + 1 :])
        if (start - low >= 2 * LANES and left >= 2 * LANES) or left == 0:
            runs.append((low, start - low, members))
            low, members = start, []
    return runs


def hidden_loads(blocks, weights, tokens, held, semaphores):
    places = [held.at[i] for i in range(len(weights))]
    parts = fetch(weights[:1], places[:1], semaphores, len(blocks))
    loads = fetch(blocks, row_views(tokens, blocks), semaphores)
    parts += fetch(weights[1:], places[1:], semaphores, len(blocks) + 1)
    pending = dict(enumerate(loads + parts))

    def ready(numbers):
        for number in numbers:
            if number in pending:
                pending.pop(number).wait()

    return ready


def hidden_tile(ready, tokens, held, pair, run, block_total):
    start, count, members = run
    ready([block_total + 2 * pair] + list(members))
    rows = tokens[start : start + count, :]
    gate_part = jnp.dot(rows, held[2 * pair], preferred_element_type=F32)
    ready([block_total + 2 * pair + 1])
    up_part = jnp.dot(rows, held[2 * pair + 1], preferred_element_type=F32)
    return gate_part / (1.0 + jnp.exp(-gate_part)) * up_part


def early_kernel(block_total, *refs):
    blocks, weights, (out, tokens, held, semaphores) = refs[:block_total], refs[block_total:-4], refs[-4:]
    ready = hidden_loads(blocks, weights, tokens, held, semaphores)
    width = held.shape[2]
    for pair in range(len(weights) // 2):
        for run in tiles_of(blocks):
            value = hidden_tile(ready, tokens, held, pair, run, block_total)
            out[run[0] : run[0] + run[1], pair * width : (pair + 1) * width] = value.astype(BF16)


def early_hidden(blocks, weights):
    count, depth = sum(b.shape[0] for b in blocks), blocks[0].shape[1]
    width, total = weights[0].shape[1], len(weights)
    return pl.pallas_call(
        functools.partial(early_kernel, len(blocks)),
        out_shape=jax.ShapeDtypeStruct((count, total // 2 * width), BF16),
        in_specs=[pl.BlockSpec(memory_space=pltpu.HBM)] * (len(blocks) + total),
        out_specs=pl.BlockSpec(memory_space=pltpu.VMEM),
        scratch_shapes=[
            pltpu.VMEM((count, depth), BF16),
            pltpu.VMEM((total, depth, width), BF16),
            pltpu.SemaphoreType.DMA((len(blocks) + total,)),
        ],
        compiler_params=WHOLE,
        cost_estimate=pl.CostEstimate(
            flops=2 * total * count * depth * width,
            bytes_accessed=2 * total * depth * width,
            transcendentals=0,
        ),
    )(*blocks, *weights)


def down_loads(tp_size, index_ref, downs, held, semaphores):
    quarter = downs[0].shape[0] // tp_size
    copies = []
    for j, ref in enumerate(downs):
        sources = [
            ref.at[pl.ds(pl.multiple_of((index_ref[0] ^ k) * quarter, LANES), quarter)]
            for k in range(tp_size)
        ]
        targets = [held.at[j, pl.ds(k * quarter, quarter)] for k in range(tp_size)]
        copies.append(fetch(sources, targets, semaphores, j * tp_size))
    return copies


def down_into(copies, hidden, held, outs):
    width, rows = held.shape[2], outs[0].shape[0]
    blocks, tile = hidden.shape[0] // rows, hidden.shape[0] // 2
    for j, group in enumerate(copies):
        for copy in group:
            copy.wait()
        for low in range(0, hidden.shape[0], tile):
            value = jnp.dot(hidden[low : low + tile, :], held[j], preferred_element_type=F32)
            value = value.astype(BF16)
            for b in range(tile // rows):
                out = outs[j // 2 * blocks + low // rows + b]
                out[:, j % 2 * width : (j % 2 + 1) * width] = value[b * rows : (b + 1) * rows, :]


def late_kernel(tp_size, block_total, late_total, index_ref, near, far, scales, *refs):
    tokens, held, semaphores, down_held, down_semaphores = refs[-5:]
    blocks, down_total = refs[:block_total], down_held.shape[0]
    weights = refs[block_total : block_total + held.shape[0]]
    low = block_total + held.shape[0]
    downs, hidden, outs = refs[low : low + down_total], refs[low + down_total], refs[low + down_total + 1 : -5]
    copies = down_loads(tp_size, index_ref, downs, down_held, down_semaphores)
    ready = hidden_loads(blocks, weights, tokens, held, semaphores)
    width, runs = held.shape[2], tiles_of(blocks)
    total, pairs = tokens.shape[0], len(weights) // 2
    tail = sum(block.shape[0] for block in blocks[-late_total:])
    last = (total - tail, tail, range(block_total - late_total, block_total))

    def put(low, value, column):
        count, extent = value.shape
        scaled = (value * scales[low : low + count, :]).astype(BF16)
        hidden[low : low + count, column : column + extent] = scaled

    put(0, near[...].astype(F32), 0)
    put(near.shape[0], far[...].astype(F32), 0)
    middle = near.shape[1]
    for pair in range(pairs):
        if pair * width < middle:
            for run in runs:
                value = hidden_tile(ready, tokens, held, pair, run, block_total)
                put(run[0], value, middle + pair * width)
        else:
            value = hidden_tile(ready, tokens, held, pair, last, block_total)
            put(last[0], value, pair * width - middle)
    down_into(copies, hidden, down_held, outs)


def late_hidden(tp_size, index, blocks, late_total, near, far, scales, weights, early_weights, downs, rows):
    count, depth = sum(b.shape[0] for b in blocks), blocks[0].shape[1]
    width, total = weights[0].shape[1], len(weights) + len(early_weights)
    vmem, from_hbm = pl.BlockSpec(memory_space=pltpu.VMEM), pl.BlockSpec(memory_space=pltpu.HBM)
    result = jax.ShapeDtypeStruct((rows, len(downs) * downs[0].shape[1]), BF16)
    outs = pl.pallas_call(
        functools.partial(late_kernel, tp_size, len(blocks), late_total),
        out_shape=(jax.ShapeDtypeStruct((count, total // 2 * width), BF16),)
        + (result,) * (count // rows),
        in_specs=[pl.BlockSpec(memory_space=pltpu.SMEM)]
        + [vmem] * 3
        + [from_hbm] * (len(blocks) + total + len(downs)),
        out_specs=(vmem,) * (1 + count // rows),
        scratch_shapes=[
            pltpu.VMEM((count, depth), BF16),
            pltpu.VMEM((total, depth, width), BF16),
            pltpu.SemaphoreType.DMA((len(blocks) + total,)),
            pltpu.VMEM((len(downs),) + downs[0].shape, BF16),
            pltpu.SemaphoreType.DMA((len(downs) * tp_size,)),
        ],
        compiler_params=WHOLE,
        cost_estimate=pl.CostEstimate(
            flops=3 * len(weights) * count * depth * width,
            bytes_accessed=2 * total * depth * width,
            transcendentals=0,
        ),
    )(index, near, far, scales, *blocks, *weights, *early_weights, *downs)
    return outs[0], outs[1:]


def down_kernel(tp_size, index_ref, hidden_ref, *refs):
    hidden, loaded, held, semaphores = refs[-4:]
    down_total = held.shape[0]
    downs, outs = refs[:down_total], refs[down_total:-4]
    copies = down_loads(tp_size, index_ref, downs[:1], held, semaphores)
    whole = pltpu.make_async_copy(hidden_ref, hidden, loaded)
    whole.start()
    for j in range(1, down_total):
        copies += down_loads(
            tp_size, index_ref, downs[j : j + 1], held.at[j : j + 1], semaphores.at[j * tp_size :]
        )
    whole.wait()
    down_into(copies, hidden, held, outs)


def down_results(tp_size, index, hidden, downs, rows):
    count, (depth, width) = hidden.shape[0], downs[0].shape
    from_hbm, total = pl.BlockSpec(memory_space=pltpu.HBM), len(downs) // 2 * (count // rows)
    outs = pl.pallas_call(
        functools.partial(down_kernel, tp_size),
        out_shape=(jax.ShapeDtypeStruct((rows, 2 * width), BF16),) * total,
        in_specs=[pl.BlockSpec(memory_space=pltpu.SMEM)] + [from_hbm] * (1 + len(downs)),
        out_specs=(pl.BlockSpec(memory_space=pltpu.VMEM),) * total,
        scratch_shapes=[
            pltpu.VMEM(hidden.shape, BF16),
            pltpu.SemaphoreType.DMA,
            pltpu.VMEM((len(downs), depth, width), BF16),
            pltpu.SemaphoreType.DMA((len(downs) * tp_size,)),
        ],
        compiler_params=WHOLE,
        cost_estimate=pl.CostEstimate(
            flops=2 * len(downs) * count * depth * width,
            bytes_accessed=2 * len(downs) * depth * width,
            transcendentals=0,
        ),
    )(index, hidden, *downs)
    return outs


def places_of(index_ref, kept, rows, shape, axis):
    spot = lax.broadcasted_iota(jnp.int32, shape, axis)
    place = spot
    for j, k in enumerate(kept):
        inside = (spot >= j * rows) & (spot < (j + 1) * rows)
        place = jnp.where(inside, spot + ((index_ref[0] ^ k) - j) * rows, place)
    return place.astype(F32)


def halves(value):
    high = value.astype(BF16)
    return high, (value - high.astype(F32)).astype(BF16)


def product(first, second, dims):
    dims = (dims, ((), ()))
    high, low = halves(first)
    exact = second.dtype == BF16
    others = (second,) if exact else halves(second)
    pairs = [(low, others[0]), (high, others[0])] if exact else [
        (low, others[0]),
        (high, others[1]),
        (high, others[0]),
    ]
    return sum(lax.dot_general(a, b, dims, preferred_element_type=F32) for a, b in pairs)


def retain_kernel(kept, *refs):
    block_total, size = len(kept), HD
    index_ref, rates = refs[:2]
    blocks, weights = refs[2 : 2 + block_total], refs[2 + block_total : 5 + block_total]
    cosine, sine_part, nearby, scaled, summary, rows, held, semaphores = refs[5 + block_total :]
    count = rows.shape[0]
    loads = fetch(blocks, row_views(rows, blocks), semaphores)
    parts = fetch(weights, [held.at[i] for i in range(3)], semaphores, block_total)
    for copy in loads:
        copy.wait()

    def projected(i):
        parts[i].wait()
        value = jnp.dot(rows[...], held[i], preferred_element_type=F32)
        return value.astype(BF16)

    def turned(value):
        value = value.astype(F32)
        return value * cosine[...] + pltpu.roll(value, size // 2, 1) * sine_part[...]

    queries, keys, values = (projected(i) for i in range(3))
    down = places_of(index_ref, kept, count // block_total, (count, 1), 0)
    offsets = down - places_of(index_ref, kept, count // block_total, (1, count), 1)
    for h in range(summary.shape[0]):
        lanes = slice(h * size, (h + 1) * size)
        rate = rates[h]
        query = turned(queries[:, lanes]) * size ** (-0.5)
        key, value = turned(keys[:, lanes]), values[:, lanes]
        decay = jnp.where(offsets >= 0, jnp.exp(-rate * jnp.maximum(offsets, 0.0)), 0.0)
        scores = decay * product(query, key, ((1,), (1,)))
        nearby[h] = product(scores, value, ((1,), (0,)))
        scaled[h] = query * jnp.exp(-rate * (down + 1.0))
        summary[h] = product(key * jnp.exp(-rate * (count - 1.0 - down)), value, ((0,), (0,)))


def retain_group(kept, index, blocks, weights, rates, cosine, sine_part):
    count, depth = sum(b.shape[0] for b in blocks), blocks[0].shape[1]
    width, heads = weights[0].shape[1], rates.shape[0]
    smem, vmem = pl.BlockSpec(memory_space=pltpu.SMEM), pl.BlockSpec(memory_space=pltpu.VMEM)
    from_hbm = pl.BlockSpec(memory_space=pltpu.HBM)
    return pl.pallas_call(
        functools.partial(retain_kernel, kept),
        out_shape=(
            jax.ShapeDtypeStruct((heads, count, HD), F32),
            jax.ShapeDtypeStruct((heads, count, HD), F32),
            jax.ShapeDtypeStruct((heads, HD, HD), F32),
        ),
        in_specs=[smem, smem] + [from_hbm] * (len(blocks) + 3) + [vmem] * 2,
        out_specs=(vmem,) * 3,
        scratch_shapes=[
            pltpu.VMEM((count, depth), BF16),
            pltpu.VMEM((3, depth, width), BF16),
            pltpu.SemaphoreType.DMA((len(blocks) + 3,)),
        ],
        compiler_params=WHOLE,
        cost_estimate=pl.CostEstimate(
            flops=8 * count * depth * width, bytes_accessed=6 * depth * width, transcendentals=0
        ),
    )(index, rates, *blocks, *weights, cosine, sine_part)


def close_kernel(nearby, scaled, state, out_weight, low, high):
    mixed = []
    for h in range(state.shape[0]):
        retained = nearby[h] + product(scaled[h], state[h], ((1,), (0,)))
        mean = jnp.mean(retained * retained, axis=-1, keepdims=True)
        mixed.append((retained * lax.rsqrt(mean + NORM_EPS)).astype(BF16))
    mixed = jnp.concatenate(mixed, axis=1)
    half = mixed.shape[0] // 2
    for out, rows in ((low, mixed[:half]), (high, mixed[half:])):
        out[...] = jnp.dot(rows, out_weight[...], preferred_element_type=F32).astype(BF16)


def close_group(nearby, scaled, state, out_weight):
    half, depth = nearby.shape[1] // 2, out_weight.shape[1]
    vmem = pl.BlockSpec(memory_space=pltpu.VMEM)
    return pl.pallas_call(
        close_kernel,
        out_shape=(jax.ShapeDtypeStruct((half, depth), BF16),) * 2,
        in_specs=[vmem] * 4,
        out_specs=(vmem,) * 2,
        compiler_params=WHOLE,
        cost_estimate=pl.CostEstimate(
            flops=4 * half * depth * out_weight.shape[0], bytes_accessed=0, transcendentals=0
        ),
    )(nearby, scaled, state, out_weight)


def mixer(mixer_blocks, query_weight, key_weight, value_weight, out_weight, decay_rate):
    own_count = mixer_blocks[0].shape[0]
    block_count = len(mixer_blocks)
    group_count = own_count * block_count
    tp_index = lax.axis_index("tp")
    kept = [k for k in range(block_count) if not k & 1] + [k for k in range(block_count) if k & 1]
    inner = jnp.concatenate(
        [(tp_index ^ k) * own_count + jnp.arange(own_count, dtype=jnp.int32) for k in kept]
    )
    positions = (lax.axis_index("ep") * group_count + inner).astype(F32)
    inverse = ROPE_BASE ** (-jnp.arange(0, HD, 2, dtype=F32) / HD)
    angles = positions[:, None] * inverse[None, :]
    cosine, sine_part = jnp.cos(angles), jnp.sin(angles)
    nearby, scaled, summary = retain_group(
        kept,
        tp_index.reshape(1),
        [mixer_blocks[k] for k in kept],
        (query_weight, key_weight, value_weight),
        decay_rate,
        jnp.concatenate([cosine, cosine], axis=1),
        jnp.concatenate([-sine_part, sine_part], axis=1),
    )
    incoming = state_before(summary, decay_rate, group_count)
    low, high = close_group(nearby, scaled, incoming, out_weight)
    arrived = exchange(high, 1)
    rows = [slice(j * own_count, (j + 1) * own_count) for j in range(block_count // 2)]
    terms = {2 * j: [low[r], arrived[r]] for j, r in enumerate(rows)}

    def added(values):
        return sum(value.astype(F32) for value in values)

    step = 2
    while step < block_count:
        terms = {
            k: terms[k] + [exchange(added(terms[k | step]).astype(BF16), step)]
            for k in terms
            if not k & step
        }
        step *= 2
    return added(terms[0])


def dense_shards(
    mixer_input,
    expert_input,
    mixer_gain,
    expert_gain,
    query_weight,
    key_weight,
    value_weight,
    out_weight,
    decay_rate,
    routing,
    route_weight,
    gate_weight,
    up_weight,
    down_weight,
    shared_gate,
    shared_up,
    shared_down,
):
    own_count = mixer_input.shape[0]
    tp_index = lax.axis_index("tp")
    ep_size, tp_size = lax.axis_size("ep"), lax.axis_size("tp")
    own_rows = norm_rows(expert_input, expert_gain)
    mixer_blocks = tp_blocks(norm_rows(mixer_input, mixer_gain))
    offsets, blocks = ring_gather(own_rows)
    gates, ups = tp_blocks(gate_weight[0]), tp_blocks(up_weight[0])
    downs = tp_blocks(down_weight[0])
    shared_rows = tp_blocks(own_rows)

    own_routes = lax.dynamic_slice_in_dim(routing, tp_index * own_count, own_count, 0)
    own_weights = lax.dynamic_slice_in_dim(route_weight, tp_index * own_count, own_count, 0)
    named = own_routes[None] == jnp.arange(ep_size, dtype=jnp.int32)[:, None, None]
    by_expert = jnp.sum(jnp.where(named, own_weights[None], 0.0), axis=2)
    by_source = lax.all_to_all(by_expert, "ep", split_axis=0, concat_axis=0, tiled=True)
    order = jnp.array(ring_order(ep_size), jnp.int32)
    ep_index = lax.axis_index("ep")
    place = jnp.where(ep_index % 2 == 0, ep_index // 2, ep_size - 1 - ep_index // 2)
    sources = order[(place + jnp.array(offsets, jnp.int32)) % ep_size]
    scales = by_source[sources].reshape(-1, 1)

    mixer_output = mixer(
        mixer_blocks, query_weight, key_weight, value_weight, out_weight, decay_rate
    )

    first, middle = 3, ep_size - 1
    weights = [w for pair in zip(gates, ups) for w in pair]
    near = early_hidden(blocks[:first], weights[:4])
    far = early_hidden(blocks[first:middle], weights[:4])
    hidden, own_results = late_hidden(
        tp_size,
        tp_index.reshape(1),
        blocks,
        len(blocks) - middle,
        near,
        far,
        scales,
        weights[4:],
        weights[:4],
        downs[:2],
        own_count,
    )
    other_results = down_results(tp_size, tp_index.reshape(1), hidden, downs[2:], own_count)
    results = (own_results, other_results)
    finals = {}
    for first, way in ((0, 1), (2, -1)):
        parts = [results[first // 2][offsets.index(d)] for d in range(ep_size)]
        total = ring_scatter(parts, way)
        width = total.shape[1] // 2
        for n in range(2):
            piece, k = total[:, n * width : (n + 1) * width], first + n
            finals[k] = piece if k == 0 else exchange(piece, k)

    shared_hidden = gated(jnp.concatenate(shared_rows, axis=0), shared_gate, shared_up)

    pieces, step = {0: shared_hidden}, tp_size // 2
    while step >= 1:
        sent = jnp.concatenate([pieces[m] for m in sorted(pieces)], axis=1)
        arrived = exchange(sent, step)
        width = shared_hidden.shape[1]
        for n, m in enumerate(sorted(pieces)):
            pieces[m | step] = arrived[:, n * width : (n + 1) * width]
        step //= 2
    columns = [
        jnp.concatenate(
            [pieces[m][(k ^ m) * own_count : ((k ^ m) + 1) * own_count] for k in range(tp_size)]
        )
        for m in range(tp_size)
    ]
    shared_result = jnp.dot(
        natural(columns, tp_index, 1), shared_down, preferred_element_type=F32
    )
    outputs = [
        finals[k].astype(F32) + shared_result[k * own_count : (k + 1) * own_count]
        for k in range(tp_size)
    ]
    return (mixer_output, natural(outputs, tp_index, 0))


def shards(*arrays):
    own_count, pick_count = arrays[0].shape[0], arrays[9].shape[1]
    per_device = arrays[11].shape[0]
    ep_size, tp_size = lax.axis_size("ep"), lax.axis_size("tp")
    capacity = (3 * own_count * pick_count + 2 * ep_size - 1) // (2 * ep_size)
    dense = per_device == 1 and 2 * capacity >= own_count
    if dense and ep_size == 8 and tp_size == 4:
        return dense_shards(*arrays)
    return routed_shards(*arrays)


def solution(mesh):
    return jax.shard_map(
        shards,
        mesh=mesh,
        in_specs=(
            P(("ep", "tp"), None),
            P(("ep", "tp"), None),
            P(),
            P(),
            P(None, "tp"),
            P(None, "tp"),
            P(None, "tp"),
            P("tp", None),
            P("tp"),
            P("ep", None),
            P("ep", None),
            P("ep", None, "tp"),
            P("ep", None, "tp"),
            P("ep", None, "tp"),
            P(None, "tp"),
            P(None, "tp"),
            P(None, "tp"),
        ),
        out_specs=(P(("ep", "tp"), None), P("ep", "tp")),
        check_vma=False,
    )
```

```python
import functools

import jax
import jax.numpy as jnp
from jax import lax
from jax.experimental import pallas as pl
from jax.experimental.pallas import tpu as pltpu
from jax.sharding import PartitionSpec as P


HD = 128
BLK = 64


NORM_EPS = 1e-06
ROPE_BASE = 10000.0
EXACT_MATMUL = lax.Precision.HIGHEST


def prefix(part, axis, combine, identity):
    place = lax.axis_index(axis)
    gathered = jax.tree.map(lambda a: lax.all_gather(a, axis), part)
    state = jax.tree.map(lambda a, e: jnp.zeros_like(a) + jnp.asarray(e, a.dtype), part, identity)

    def one(turn, state):
        return combine(
            state, jax.tree.map(lambda a: lax.dynamic_index_in_dim(a, turn, 0, False), gathered)
        )

    return lax.fori_loop(0, place, one, state)


def norm_rows(inputs, gain_vector):
    values = inputs.astype(jnp.float32)
    scaled = values * lax.rsqrt(jnp.mean(values * values, axis=-1, keepdims=True) + NORM_EPS)
    return (scaled * gain_vector).astype(jnp.bfloat16)


def rotate(head_rows, positions):
    head_size = head_rows.shape[-1]
    inverse = ROPE_BASE ** (-jnp.arange(0, head_size, 2, dtype=jnp.float32) / head_size)
    angles = positions[:, None] * inverse[None, :]
    cosine = jnp.cos(angles)[:, None, :]
    sine_part = jnp.sin(angles)[:, None, :]
    front_half = head_rows[..., : head_size // 2]
    behind = head_rows[..., head_size // 2 :]
    return jnp.concatenate(
        [front_half * cosine - behind * sine_part, front_half * sine_part + behind * cosine],
        axis=-1,
    )


def project(inputs, weight, head_total):
    product = jnp.dot(inputs, weight, preferred_element_type=jnp.float32).astype(jnp.bfloat16)
    product = lax.optimization_barrier(product)
    return product.astype(jnp.float32).reshape(inputs.shape[0], head_total, -1)


def chain_combine(earlier, latter):
    return (earlier[0] * latter[0], latter[0][:, None, None] * earlier[1] + latter[1])


def retain_local(query_heads, key_heads, value_heads, decay_rates):
    length, head_total, head_size = query_heads.shape
    blocks = length // BLK
    log_gamma = -decay_rates
    inner_pos = jnp.arange(BLK, dtype=jnp.float32)
    offsets = inner_pos[:, None] - inner_pos[None, :]
    inside_block_output = jnp.where(
        offsets >= 0, jnp.exp(log_gamma[:, None, None] * jnp.maximum(offsets, 0.0)), 0.0
    )
    key_scale = jnp.exp(log_gamma[None, :] * (BLK - 1.0 - inner_pos)[:, None])
    query_scale = jnp.exp(log_gamma[None, :] * (inner_pos + 1.0)[:, None])
    blocked = (blocks, BLK, head_total, head_size)
    q_blocks = query_heads.reshape(blocked)
    k_blocks = key_heads.reshape(blocked)
    v_blocks = value_heads.reshape(blocked)
    attention_scores = (
        jnp.einsum("nchd,nmhd->nhcm", q_blocks, k_blocks, precision=EXACT_MATMUL)
        * inside_block_output[None]
    )
    nearby = jnp.einsum("nhcm,nmhe->nche", attention_scores, v_blocks, precision=EXACT_MATMUL)
    block_states = jnp.einsum(
        "nchd,nche->nhde", k_blocks * key_scale[None, :, :, None], v_blocks, precision=EXACT_MATMUL
    )
    block_offset_rows = jnp.arange(blocks, dtype=jnp.float32)
    to_end = jnp.exp(log_gamma[None, :] * BLK * (blocks - 1.0 - block_offset_rows)[:, None])
    summary = jnp.einsum("nh,nhde->hde", to_end, block_states, precision=EXACT_MATMUL)
    through = jnp.exp(log_gamma * (BLK * blocks))
    incoming = prefix(
        (through, summary), "ep", chain_combine, (jnp.ones_like(through), jnp.zeros_like(summary))
    )[1]
    block_gaps = block_offset_rows[:, None] - 1.0 - block_offset_rows[None, :]
    carry_mix = jnp.where(
        block_gaps >= 0, jnp.exp(log_gamma[:, None, None] * BLK * jnp.maximum(block_gaps, 0.0)), 0.0
    )
    entering = jnp.einsum("hbj,jhde->bhde", carry_mix, block_states, precision=EXACT_MATMUL)
    entering = (
        entering
        + jnp.exp(log_gamma[None, :] * BLK * block_offset_rows[:, None])[:, :, None, None]
        * incoming[None]
    )
    distant = jnp.einsum(
        "bchd,bhde->bche",
        q_blocks * query_scale[None, :, :, None],
        entering,
        precision=EXACT_MATMUL,
    )
    retained = (nearby + distant).reshape(length, head_total, head_size)
    normed = retained * lax.rsqrt(jnp.mean(retained * retained, axis=-1, keepdims=True) + NORM_EPS)
    return normed.astype(jnp.bfloat16).reshape(length, head_total * head_size)


def assign_slots(routes, source_rows, capacity, expert_count):
    token_count, pick_count = routes.shape
    chosen = routes.reshape(token_count * pick_count)
    onehot = (chosen[:, None] == jnp.arange(expert_count, dtype=jnp.int32)[None, :]).astype(
        jnp.int32
    )
    per_source = onehot.reshape(token_count // source_rows, source_rows * pick_count, expert_count)
    earlier_hits = jnp.cumsum(per_source, axis=1) - per_source
    ranks = jnp.sum(earlier_hits * per_source, axis=2).reshape(token_count * pick_count)
    sources = jnp.arange(token_count * pick_count, dtype=jnp.int32) // (source_rows * pick_count)
    return (chosen, sources * capacity + ranks)


def gather_slots(token_rows, chosen, slot_ids, slot_count, expert_count, pick_count):
    owners = jnp.arange(chosen.shape[0], dtype=jnp.int32) // pick_count + 1
    owner_table = jnp.zeros((slot_count, expert_count), jnp.int32).at[slot_ids, chosen].set(owners)
    padded = jnp.concatenate(
        [jnp.zeros((1, token_rows.shape[1]), token_rows.dtype), token_rows], axis=0
    )
    return padded[owner_table]


def expert_hidden(routed_rows, gate_weight, up_weight):
    per_device = gate_weight.shape[0]
    grouped = routed_rows.reshape(
        routed_rows.shape[0], routed_rows.shape[1] // per_device, per_device, routed_rows.shape[2]
    )
    gate_part = jnp.einsum(
        "snxd,xdf->snxf", grouped, gate_weight, preferred_element_type=jnp.float32
    )
    up_part = jnp.einsum("snxd,xdf->snxf", grouped, up_weight, preferred_element_type=jnp.float32)
    return (jax.nn.silu(gate_part) * up_part).astype(jnp.bfloat16)


def routed_shards(
    mixer_input,
    expert_input,
    mixer_gain,
    expert_gain,
    query_weight,
    key_weight,
    value_weight,
    out_weight,
    decay_rate,
    routing,
    route_weight,
    gate_weight,
    up_weight,
    down_weight,
    shared_gate,
    shared_up,
    shared_down,
):
    own_count = mixer_input.shape[0]
    tp_index = lax.axis_index("tp")
    own_expert_rows = norm_rows(expert_input, expert_gain)
    mixer_rows, expert_rows = (
        lax.all_gather(norm_rows(mixer_input, mixer_gain), "tp", axis=0, tiled=True),
        lax.all_gather(own_expert_rows, "tp", axis=0, tiled=True),
    )
    group_count = mixer_rows.shape[0]
    head_total = decay_rate.shape[0]
    positions = (
        lax.axis_index("ep") * group_count + jnp.arange(group_count, dtype=jnp.int32)
    ).astype(jnp.float32)
    query_heads = rotate(project(mixer_rows, query_weight, head_total), positions) * HD ** (-0.5)
    key_heads = rotate(project(mixer_rows, key_weight, head_total), positions)
    value_heads = project(mixer_rows, value_weight, head_total)
    mixed_heads = retain_local(query_heads, key_heads, value_heads, decay_rate)
    mixer_output = lax.psum_scatter(
        jnp.dot(mixed_heads, out_weight, preferred_element_type=jnp.float32).astype(jnp.bfloat16),
        "tp",
        scatter_dimension=0,
        tiled=True,
    ).astype(jnp.float32)
    expert_count = lax.axis_size("ep") * gate_weight.shape[0]
    pick_count = routing.shape[1]
    capacity = (3 * own_count * pick_count + 2 * expert_count - 1) // (2 * expert_count)
    chosen, slot_ids = assign_slots(routing, own_count, capacity, expert_count)
    own_span = own_count * pick_count
    own_chosen = lax.dynamic_slice_in_dim(chosen, tp_index * own_span, own_span, 0)
    own_slots = (
        lax.dynamic_slice_in_dim(slot_ids, tp_index * own_span, own_span, 0) - tp_index * capacity
    )
    outgoing = gather_slots(
        own_expert_rows, own_chosen, own_slots, capacity, expert_count, pick_count
    )
    arrived = lax.all_to_all(outgoing, "ep", split_axis=1, concat_axis=1, tiled=True)
    hidden = expert_hidden(
        lax.all_gather(arrived, "tp", axis=0, tiled=True), gate_weight, up_weight
    )
    shared_hidden = (
        jax.nn.silu(jnp.dot(expert_rows, shared_gate, preferred_element_type=jnp.float32))
        * jnp.dot(expert_rows, shared_up, preferred_element_type=jnp.float32)
    ).astype(jnp.bfloat16)
    full_hidden, full_shared = (
        lax.all_gather(hidden, "tp", axis=3, tiled=True),
        lax.all_gather(shared_hidden, "tp", axis=1, tiled=True),
    )
    results = jnp.einsum(
        "snxf,xfe->snxe", full_hidden, down_weight, preferred_element_type=jnp.float32
    ).astype(jnp.bfloat16)
    results = results.reshape(results.shape[0], expert_count, results.shape[3])
    returned = lax.all_to_all(results, "ep", split_axis=1, concat_axis=1, tiled=True)
    flat_results = returned.reshape(returned.shape[0] * expert_count, returned.shape[2])
    picked = flat_results[slot_ids * expert_count + chosen].astype(jnp.float32)
    weighted = jnp.sum(
        picked.reshape(group_count, pick_count, -1) * route_weight[:, :, None], axis=1
    )
    shared_result = jnp.dot(full_shared, shared_down, preferred_element_type=jnp.float32)
    expert_output = weighted + shared_result
    return (mixer_output, expert_output)


BF16, F32 = jnp.bfloat16, jnp.float32
LANES = 128
RING_STEPS, XOR_STEPS = 4, 2
WHOLE = pltpu.CompilerParams(vmem_limit_bytes=60 << 20)


def exchange(value, step):
    size = lax.axis_size("tp")
    return lax.ppermute(value, "tp", [(i, i ^ step) for i in range(size)])


def ring_order(size):
    return [i for i in range(0, size, 2)] + [i for i in range(size - 1, 0, -2)]


def ring_shift(value, step):
    size = lax.axis_size("ep")
    order = ring_order(size)
    return lax.ppermute(value, "ep", [(order[i], order[(i + step) % size]) for i in range(size)])


def tp_blocks(value):
    held = {0: value}
    step = lax.axis_size("tp") // 2
    while step >= 1:
        for k in list(held):
            held[k | step] = exchange(held[k], step)
        step //= 2
    return [held[k] for k in range(lax.axis_size("tp"))]


def ring_gather(value):
    size = lax.axis_size("ep")
    half, rows = size // 2, value.shape[0] // 2
    offsets, blocks = [0], [value]
    ahead = behind = value
    for d in range(1, half):
        behind = ring_shift(behind, 1)
        ahead = ring_shift(ahead, -1)
        offsets += [size - d, d]
        blocks += [behind, ahead]
    offsets.append(half)
    blocks.append(ring_shift(behind[:rows], 1))
    blocks.append(ring_shift(ahead[rows:], -1))
    return offsets, blocks


def ring_scatter(parts, way):
    size = lax.axis_size("ep")
    half = size // 2
    long, short = parts[half], parts[(-way * (half - 1)) % size]

    def added(first, second):
        return (first.astype(F32) + second.astype(F32)).astype(BF16)

    for d in range(half, 0, -1):
        long = ring_shift(long, way)
        if d > 1:
            short = ring_shift(short, -way)
        if d > 1:
            long = added(long, parts[(way * (d - 1)) % size])
        if d > 2:
            short = added(short, parts[(-way * (d - 2)) % size])
    return (parts[0].astype(F32) + long.astype(F32) + short.astype(F32)).astype(BF16)


def state_before(summary, decay_rate, group_count):
    size, place = lax.axis_size("ep"), lax.axis_index("ep")
    rate = decay_rate[:, None, None] * group_count
    state, total = jnp.zeros_like(summary), summary
    step = 1
    while step < size:
        other = lax.ppermute(total, "ep", [(i, i ^ step) for i in range(size)])
        later = (place & step) != 0
        inside = (place & (step - 1)).astype(F32)
        state = state + jnp.where(later, jnp.exp(-rate * inside) * other, 0.0)
        passed = jnp.exp(-rate * step)
        total = jnp.where(later, passed * other + total, passed * total + other)
        step *= 2
    return state


def natural(blocks, tp_index, axis):
    extent = blocks[0].shape[axis]
    shape = list(blocks[0].shape)
    shape[axis] = extent * len(blocks)
    total = jnp.zeros(shape, blocks[0].dtype)
    for k, block in enumerate(blocks):
        total = lax.dynamic_update_slice_in_dim(total, block, (tp_index ^ k) * extent, axis)
    return total


def gated(rows, gate, up):
    gate_part = jnp.dot(rows, gate, preferred_element_type=F32)
    up_part = jnp.dot(rows, up, preferred_element_type=F32)
    return (jax.nn.silu(gate_part) * up_part).astype(BF16)


def fetch(sources, targets, semaphores, first=0):
    copies = [
        pltpu.make_async_copy(source, target, semaphores.at[first + i])
        for i, (source, target) in enumerate(zip(sources, targets))
    ]
    for copy in copies:
        copy.start()
    return copies


def row_views(ref, blocks, start=0):
    views = []
    for block in blocks:
        views.append(ref.at[pl.ds(start, block.shape[0])])
        start += block.shape[0]
    return views


def tiles_of(blocks):
    runs, start, low, members = [], 0, 0, []
    for number, block in enumerate(blocks):
        members.append(number)
        start += block.shape[0]
        left = sum(b.shape[0] for b in blocks[number + 1 :])
        if (start - low >= 2 * LANES and left >= 2 * LANES) or left == 0:
            runs.append((low, start - low, members))
            low, members = start, []
    return runs


def hidden_loads(blocks, weights, tokens, held, semaphores):
    places = [held.at[i] for i in range(len(weights))]
    parts = fetch(weights[:1], places[:1], semaphores, len(blocks))
    loads = fetch(blocks, row_views(tokens, blocks), semaphores)
    parts += fetch(weights[1:], places[1:], semaphores, len(blocks) + 1)
    pending = dict(enumerate(loads + parts))

    def ready(numbers):
        for number in numbers:
            if number in pending:
                pending.pop(number).wait()

    return ready


def hidden_tile(ready, tokens, held, pair, run, block_total):
    start, count, members = run
    ready([block_total + 2 * pair] + list(members))
    rows = tokens[start : start + count, :]
    gate_part = jnp.dot(rows, held[2 * pair], preferred_element_type=F32)
    ready([block_total + 2 * pair + 1])
    up_part = jnp.dot(rows, held[2 * pair + 1], preferred_element_type=F32)
    return gate_part / (1.0 + jnp.exp(-gate_part)) * up_part


def early_kernel(block_total, *refs):
    blocks, weights, (out, tokens, held, semaphores) = refs[:block_total], refs[block_total:-4], refs[-4:]
    ready = hidden_loads(blocks, weights, tokens, held, semaphores)
    width = held.shape[2]
    for pair in range(len(weights) // 2):
        for run in tiles_of(blocks):
            value = hidden_tile(ready, tokens, held, pair, run, block_total)
            out[run[0] : run[0] + run[1], pair * width : (pair + 1) * width] = value.astype(BF16)


def early_hidden(blocks, weights):
    count, depth = sum(b.shape[0] for b in blocks), blocks[0].shape[1]
    width, total = weights[0].shape[1], len(weights)
    return pl.pallas_call(
        functools.partial(early_kernel, len(blocks)),
        out_shape=jax.ShapeDtypeStruct((count, total // 2 * width), BF16),
        in_specs=[pl.BlockSpec(memory_space=pltpu.HBM)] * (len(blocks) + total),
        out_specs=pl.BlockSpec(memory_space=pltpu.VMEM),
        scratch_shapes=[
            pltpu.VMEM((count, depth), BF16),
            pltpu.VMEM((total, depth, width), BF16),
            pltpu.SemaphoreType.DMA((len(blocks) + total,)),
        ],
        compiler_params=WHOLE,
        cost_estimate=pl.CostEstimate(
            flops=2 * total * count * depth * width,
            bytes_accessed=2 * total * depth * width,
            transcendentals=0,
        ),
    )(*blocks, *weights)


def down_loads(tp_size, index_ref, downs, held, semaphores):
    quarter = downs[0].shape[0] // tp_size
    copies = []
    for j, ref in enumerate(downs):
        sources = [
            ref.at[pl.ds(pl.multiple_of((index_ref[0] ^ k) * quarter, LANES), quarter)]
            for k in range(tp_size)
        ]
        targets = [held.at[j, pl.ds(k * quarter, quarter)] for k in range(tp_size)]
        copies.append(fetch(sources, targets, semaphores, j * tp_size))
    return copies


def down_into(copies, hidden, held, outs):
    width, rows = held.shape[2], outs[0].shape[0]
    blocks, tile = hidden.shape[0] // rows, hidden.shape[0] // 2
    for j, group in enumerate(copies):
        for copy in group:
            copy.wait()
        for low in range(0, hidden.shape[0], tile):
            value = jnp.dot(hidden[low : low + tile, :], held[j], preferred_element_type=F32)
            value = value.astype(BF16)
            for b in range(tile // rows):
                out = outs[j // 2 * blocks + low // rows + b]
                out[:, j % 2 * width : (j % 2 + 1) * width] = value[b * rows : (b + 1) * rows, :]


def late_kernel(tp_size, block_total, late_total, index_ref, near, far, scales, *refs):
    tokens, held, semaphores, down_held, down_semaphores = refs[-5:]
    blocks, down_total = refs[:block_total], down_held.shape[0]
    weights = refs[block_total : block_total + held.shape[0]]
    low = block_total + held.shape[0]
    downs, hidden, outs = refs[low : low + down_total], refs[low + down_total], refs[low + down_total + 1 : -5]
    copies = down_loads(tp_size, index_ref, downs, down_held, down_semaphores)
    ready = hidden_loads(blocks, weights, tokens, held, semaphores)
    width, runs = held.shape[2], tiles_of(blocks)
    total, pairs = tokens.shape[0], len(weights) // 2
    tail = sum(block.shape[0] for block in blocks[-late_total:])
    last = (total - tail, tail, range(block_total - late_total, block_total))

    columns, rows = scales[...].T, scales.shape[1]

    def put(low, value, column):
        for start in range(0, value.shape[0], rows):
            block = (low + start) // rows
            scaled = value[start : start + rows, :] * columns[:, block : block + 1]
            hidden[low + start : low + start + rows, column : column + value.shape[1]] = (
                scaled.astype(BF16)
            )

    put(0, near[...].astype(F32), 0)
    put(near.shape[0], far[...].astype(F32), 0)
    middle = near.shape[1]
    for pair in range(pairs):
        if pair * width < middle:
            for run in runs:
                value = hidden_tile(ready, tokens, held, pair, run, block_total)
                put(run[0], value, middle + pair * width)
        else:
            value = hidden_tile(ready, tokens, held, pair, last, block_total)
            put(last[0], value, pair * width - middle)
    down_into(copies, hidden, down_held, outs)


def late_hidden(tp_size, index, blocks, late_total, near, far, scales, weights, early_weights, downs, rows):
    count, depth = sum(b.shape[0] for b in blocks), blocks[0].shape[1]
    width, total = weights[0].shape[1], len(weights) + len(early_weights)
    vmem, from_hbm = pl.BlockSpec(memory_space=pltpu.VMEM), pl.BlockSpec(memory_space=pltpu.HBM)
    result = jax.ShapeDtypeStruct((rows, len(downs) * downs[0].shape[1]), BF16)
    outs = pl.pallas_call(
        functools.partial(late_kernel, tp_size, len(blocks), late_total),
        out_shape=(jax.ShapeDtypeStruct((count, total // 2 * width), BF16),)
        + (result,) * (count // rows),
        in_specs=[pl.BlockSpec(memory_space=pltpu.SMEM)]
        + [vmem] * 3
        + [from_hbm] * (len(blocks) + total + len(downs)),
        out_specs=(vmem,) * (1 + count // rows),
        scratch_shapes=[
            pltpu.VMEM((count, depth), BF16),
            pltpu.VMEM((total, depth, width), BF16),
            pltpu.SemaphoreType.DMA((len(blocks) + total,)),
            pltpu.VMEM((len(downs),) + downs[0].shape, BF16),
            pltpu.SemaphoreType.DMA((len(downs) * tp_size,)),
        ],
        compiler_params=WHOLE,
        cost_estimate=pl.CostEstimate(
            flops=3 * len(weights) * count * depth * width,
            bytes_accessed=2 * total * depth * width,
            transcendentals=0,
        ),
    )(index, near, far, scales, *blocks, *weights, *early_weights, *downs)
    return outs[0], outs[1:]


def down_kernel(tp_size, index_ref, hidden_ref, *refs):
    hidden, loaded, held, semaphores = refs[-4:]
    down_total = held.shape[0]
    downs, outs = refs[:down_total], refs[down_total:-4]
    copies = down_loads(tp_size, index_ref, downs[:1], held, semaphores)
    whole = pltpu.make_async_copy(hidden_ref, hidden, loaded)
    whole.start()
    for j in range(1, down_total):
        copies += down_loads(
            tp_size, index_ref, downs[j : j + 1], held.at[j : j + 1], semaphores.at[j * tp_size :]
        )
    whole.wait()
    down_into(copies, hidden, held, outs)


def down_results(tp_size, index, hidden, downs, rows):
    count, (depth, width) = hidden.shape[0], downs[0].shape
    from_hbm, total = pl.BlockSpec(memory_space=pltpu.HBM), len(downs) // 2 * (count // rows)
    outs = pl.pallas_call(
        functools.partial(down_kernel, tp_size),
        out_shape=(jax.ShapeDtypeStruct((rows, 2 * width), BF16),) * total,
        in_specs=[pl.BlockSpec(memory_space=pltpu.SMEM)] + [from_hbm] * (1 + len(downs)),
        out_specs=(pl.BlockSpec(memory_space=pltpu.VMEM),) * total,
        scratch_shapes=[
            pltpu.VMEM(hidden.shape, BF16),
            pltpu.SemaphoreType.DMA,
            pltpu.VMEM((len(downs), depth, width), BF16),
            pltpu.SemaphoreType.DMA((len(downs) * tp_size,)),
        ],
        compiler_params=WHOLE,
        cost_estimate=pl.CostEstimate(
            flops=2 * len(downs) * count * depth * width,
            bytes_accessed=2 * len(downs) * depth * width,
            transcendentals=0,
        ),
    )(index, hidden, *downs)
    return outs


def places_of(index_ref, kept, rows, shape, axis):
    spot = lax.broadcasted_iota(jnp.int32, shape, axis)
    place = spot
    for j, k in enumerate(kept):
        inside = (spot >= j * rows) & (spot < (j + 1) * rows)
        place = jnp.where(inside, spot + ((index_ref[0] ^ k) - j) * rows, place)
    return place.astype(F32)


def halves(value):
    high = value.astype(BF16)
    return high, (value - high.astype(F32)).astype(BF16)


def product(first, second, dims):
    dims = (dims, ((), ()))
    high, low = halves(first)
    exact = second.dtype == BF16
    others = (second,) if exact else halves(second)
    pairs = [(low, others[0]), (high, others[0])] if exact else [
        (low, others[0]),
        (high, others[1]),
        (high, others[0]),
    ]
    return sum(lax.dot_general(a, b, dims, preferred_element_type=F32) for a, b in pairs)


def retain_kernel(kept, *refs):
    block_total, size = len(kept), HD
    index_ref, rates = refs[:2]
    blocks, weights = refs[2 : 2 + block_total], refs[2 + block_total : 5 + block_total]
    cosine, sine_part, nearby, scaled, summary, rows, held, semaphores = refs[5 + block_total :]
    count = rows.shape[0]
    loads = fetch(blocks, row_views(rows, blocks), semaphores)
    parts = fetch(weights, [held.at[i] for i in range(3)], semaphores, block_total)
    for copy in loads:
        copy.wait()

    def projected(i):
        parts[i].wait()
        value = jnp.dot(rows[...], held[i], preferred_element_type=F32)
        return value.astype(BF16)

    def turned(value):
        value = value.astype(F32)
        return value * cosine[...] + pltpu.roll(value, size // 2, 1) * sine_part[...]

    queries, keys, values = (projected(i) for i in range(3))
    down = places_of(index_ref, kept, count // block_total, (count, 1), 0)
    offsets = down - places_of(index_ref, kept, count // block_total, (1, count), 1)
    for h in range(summary.shape[0]):
        lanes = slice(h * size, (h + 1) * size)
        rate = rates[h]
        query = turned(queries[:, lanes]) * size ** (-0.5)
        key, value = turned(keys[:, lanes]), values[:, lanes]
        decay = jnp.where(offsets >= 0, jnp.exp(-rate * jnp.maximum(offsets, 0.0)), 0.0)
        scores = decay * product(query, key, ((1,), (1,)))
        nearby[h] = product(scores, value, ((1,), (0,)))
        scaled[h] = query * jnp.exp(-rate * (down + 1.0))
        summary[h] = product(key * jnp.exp(-rate * (count - 1.0 - down)), value, ((0,), (0,)))


def retain_group(kept, index, blocks, weights, rates, cosine, sine_part):
    count, depth = sum(b.shape[0] for b in blocks), blocks[0].shape[1]
    width, heads = weights[0].shape[1], rates.shape[0]
    smem, vmem = pl.BlockSpec(memory_space=pltpu.SMEM), pl.BlockSpec(memory_space=pltpu.VMEM)
    from_hbm = pl.BlockSpec(memory_space=pltpu.HBM)
    return pl.pallas_call(
        functools.partial(retain_kernel, kept),
        out_shape=(
            jax.ShapeDtypeStruct((heads, count, HD), F32),
            jax.ShapeDtypeStruct((heads, count, HD), F32),
            jax.ShapeDtypeStruct((heads, HD, HD), F32),
        ),
        in_specs=[smem, smem] + [from_hbm] * (len(blocks) + 3) + [vmem] * 2,
        out_specs=(vmem,) * 3,
        scratch_shapes=[
            pltpu.VMEM((count, depth), BF16),
            pltpu.VMEM((3, depth, width), BF16),
            pltpu.SemaphoreType.DMA((len(blocks) + 3,)),
        ],
        compiler_params=WHOLE,
        cost_estimate=pl.CostEstimate(
            flops=8 * count * depth * width, bytes_accessed=6 * depth * width, transcendentals=0
        ),
    )(index, rates, *blocks, *weights, cosine, sine_part)


def close_kernel(nearby, scaled, state, out_weight, low, high):
    mixed = []
    for h in range(state.shape[0]):
        retained = nearby[h] + product(scaled[h], state[h], ((1,), (0,)))
        mean = jnp.mean(retained * retained, axis=-1, keepdims=True)
        mixed.append((retained * lax.rsqrt(mean + NORM_EPS)).astype(BF16))
    mixed = jnp.concatenate(mixed, axis=1)
    half = mixed.shape[0] // 2
    for out, rows in ((low, mixed[:half]), (high, mixed[half:])):
        out[...] = jnp.dot(rows, out_weight[...], preferred_element_type=F32).astype(BF16)


def close_group(nearby, scaled, state, out_weight):
    half, depth = nearby.shape[1] // 2, out_weight.shape[1]
    vmem = pl.BlockSpec(memory_space=pltpu.VMEM)
    return pl.pallas_call(
        close_kernel,
        out_shape=(jax.ShapeDtypeStruct((half, depth), BF16),) * 2,
        in_specs=[vmem] * 4,
        out_specs=(vmem,) * 2,
        compiler_params=WHOLE,
        cost_estimate=pl.CostEstimate(
            flops=4 * half * depth * out_weight.shape[0], bytes_accessed=0, transcendentals=0
        ),
    )(nearby, scaled, state, out_weight)


def mixer(mixer_blocks, query_weight, key_weight, value_weight, out_weight, decay_rate):
    own_count = mixer_blocks[0].shape[0]
    block_count = len(mixer_blocks)
    group_count = own_count * block_count
    tp_index = lax.axis_index("tp")
    kept = [k for k in range(block_count) if not k & 1] + [k for k in range(block_count) if k & 1]
    inner = jnp.concatenate(
        [(tp_index ^ k) * own_count + jnp.arange(own_count, dtype=jnp.int32) for k in kept]
    )
    positions = (lax.axis_index("ep") * group_count + inner).astype(F32)
    inverse = ROPE_BASE ** (-jnp.arange(0, HD, 2, dtype=F32) / HD)
    angles = positions[:, None] * inverse[None, :]
    cosine, sine_part = jnp.cos(angles), jnp.sin(angles)
    nearby, scaled, summary = retain_group(
        kept,
        tp_index.reshape(1),
        [mixer_blocks[k] for k in kept],
        (query_weight, key_weight, value_weight),
        decay_rate,
        jnp.concatenate([cosine, cosine], axis=1),
        jnp.concatenate([-sine_part, sine_part], axis=1),
    )
    incoming = state_before(summary, decay_rate, group_count)
    low, high = close_group(nearby, scaled, incoming, out_weight)
    arrived = exchange(high, 1)
    rows = [slice(j * own_count, (j + 1) * own_count) for j in range(block_count // 2)]
    terms = {2 * j: [low[r], arrived[r]] for j, r in enumerate(rows)}

    def added(values):
        return sum(value.astype(F32) for value in values)

    step = 2
    while step < block_count:
        terms = {
            k: terms[k] + [exchange(added(terms[k | step]).astype(BF16), step)]
            for k in terms
            if not k & step
        }
        step *= 2
    return added(terms[0])


def dense_shards(
    mixer_input,
    expert_input,
    mixer_gain,
    expert_gain,
    query_weight,
    key_weight,
    value_weight,
    out_weight,
    decay_rate,
    routing,
    route_weight,
    gate_weight,
    up_weight,
    down_weight,
    shared_gate,
    shared_up,
    shared_down,
):
    own_count = mixer_input.shape[0]
    tp_index = lax.axis_index("tp")
    ep_size, tp_size = lax.axis_size("ep"), lax.axis_size("tp")
    own_rows = norm_rows(expert_input, expert_gain)
    mixer_blocks = tp_blocks(norm_rows(mixer_input, mixer_gain))
    offsets, blocks = ring_gather(own_rows)
    gates, ups = tp_blocks(gate_weight[0]), tp_blocks(up_weight[0])
    downs = tp_blocks(down_weight[0])
    shared_rows = tp_blocks(own_rows)

    own_routes = lax.dynamic_slice_in_dim(routing, tp_index * own_count, own_count, 0)
    own_weights = lax.dynamic_slice_in_dim(route_weight, tp_index * own_count, own_count, 0)
    named = own_routes[None] == jnp.arange(ep_size, dtype=jnp.int32)[:, None, None]
    by_expert = jnp.sum(jnp.where(named, own_weights[None], 0.0), axis=2)
    by_source = lax.all_to_all(by_expert, "ep", split_axis=0, concat_axis=0, tiled=True)
    order = jnp.array(ring_order(ep_size), jnp.int32)
    ep_index = lax.axis_index("ep")
    place = jnp.where(ep_index % 2 == 0, ep_index // 2, ep_size - 1 - ep_index // 2)
    sources = order[(place + jnp.array(offsets, jnp.int32)) % ep_size]
    scales = by_source[sources].reshape(len(offsets), own_count)

    mixer_output = mixer(
        mixer_blocks, query_weight, key_weight, value_weight, out_weight, decay_rate
    )

    first, middle = 3, ep_size - 1
    weights = [w for pair in zip(gates, ups) for w in pair]
    near = early_hidden(blocks[:first], weights[:4])
    far = early_hidden(blocks[first:middle], weights[:4])
    hidden, own_results = late_hidden(
        tp_size,
        tp_index.reshape(1),
        blocks,
        len(blocks) - middle,
        near,
        far,
        scales,
        weights[4:],
        weights[:4],
        downs[:2],
        own_count,
    )
    other_results = down_results(tp_size, tp_index.reshape(1), hidden, downs[2:], own_count)
    results = (own_results, other_results)
    finals = {}
    for first, way in ((0, 1), (2, -1)):
        parts = [results[first // 2][offsets.index(d)] for d in range(ep_size)]
        total = ring_scatter(parts, way)
        width = total.shape[1] // 2
        for n in range(2):
            piece, k = total[:, n * width : (n + 1) * width], first + n
            finals[k] = piece if k == 0 else exchange(piece, k)

    shared_hidden = gated(jnp.concatenate(shared_rows, axis=0), shared_gate, shared_up)

    pieces, step = {0: shared_hidden}, tp_size // 2
    while step >= 1:
        sent = jnp.concatenate([pieces[m] for m in sorted(pieces)], axis=1)
        arrived = exchange(sent, step)
        width = shared_hidden.shape[1]
        for n, m in enumerate(sorted(pieces)):
            pieces[m | step] = arrived[:, n * width : (n + 1) * width]
        step //= 2
    columns = [
        jnp.concatenate(
            [pieces[m][(k ^ m) * own_count : ((k ^ m) + 1) * own_count] for k in range(tp_size)]
        )
        for m in range(tp_size)
    ]
    shared_result = jnp.dot(
        natural(columns, tp_index, 1), shared_down, preferred_element_type=F32
    )
    outputs = [
        finals[k].astype(F32) + shared_result[k * own_count : (k + 1) * own_count]
        for k in range(tp_size)
    ]
    return (mixer_output, natural(outputs, tp_index, 0))


def shards(*arrays):
    own_count, pick_count = arrays[0].shape[0], arrays[9].shape[1]
    per_device = arrays[11].shape[0]
    ep_size, tp_size = lax.axis_size("ep"), lax.axis_size("tp")
    capacity = (3 * own_count * pick_count + 2 * ep_size - 1) // (2 * ep_size)
    dense = per_device == 1 and 2 * capacity >= own_count
    if dense and ep_size == 2 * RING_STEPS and tp_size == 2**XOR_STEPS:
        return dense_shards(*arrays)
    return routed_shards(*arrays)


def solution(mesh):
    return jax.shard_map(
        shards,
        mesh=mesh,
        in_specs=(
            P(("ep", "tp"), None),
            P(("ep", "tp"), None),
            P(),
            P(),
            P(None, "tp"),
            P(None, "tp"),
            P(None, "tp"),
            P("tp", None),
            P("tp"),
            P("ep", None),
            P("ep", None),
            P("ep", None, "tp"),
            P("ep", None, "tp"),
            P("ep", None, "tp"),
            P(None, "tp"),
            P(None, "tp"),
            P(None, "tp"),
        ),
        out_specs=(P(("ep", "tp"), None), P("ep", "tp")),
        check_vma=False,
    )
```
